32 devices in a mesh: st: 4 (over y, x), tp: 8 (over z, core).
Axes of the slice: x: 2, y: 2, z: 4, core: 2. Of those that a mesh axis runs over, the one named last changes fastest.
Arguments:
- normed: bfloat16 [2048, 2048], P('st'), may hold values from -128 to 128
- store: bfloat16 [8192, 2048], P('st'), may hold values from -5 to 5
- passage_ids: int32 [16, 2], P('st'), may hold values from 0 to 127, as said below
- w_query: bfloat16 [2048, 2048], P(None, 'tp'), as said below
- w_gate: bfloat16 [2048, 2048], P(None, 'tp'), may hold values from -0.125 to 0.125
- w_key: bfloat16 [2048, 2048], P(None, 'tp'), as said below
- w_value: bfloat16 [2048, 2048], P(None, 'tp'), may hold values from -0.125 to 0.125
- cotangent: bfloat16 [2048, 2048], P('st', 'tp'), may hold values from -6 to 6
Outputs:
- grad_rows: float32 [2048, 2048], P('st', 'tp')
- grad_store: float32 [8192, 2048], P('st', 'tp')
- grad_query_weight: float32 [2048, 2048], P('st', 'tp')
The draws below stay inside these ranges and needn't reach their ends.
Inputs may be any that keep to these rules, and one draw needn't show every extreme that they name: `passage_ids`: each row names 2 passages. The passages read by the blocks of one index of st are all different, and at most 4 of them belong to any one owner (the owner of passage p is the index p // 32 of st). In every draw some owner has one of its passages read by every index of st. `w_query`: entries lie within 6 * 2048 ** -0.5 in magnitude. `w_key`: entries lie within 8 * 2048 ** -0.5 in magnitude.
All inputs are finite; a program needn't handle non-finite values.
Results may differ from the reference program's by a relative error of at most 0.019.
Values may be sent and summed in bfloat16 or wider, within the bound.
A program may use at most 128 MiB of HBM per device.

```python
import jax
import jax.numpy as jnp
from jax import lax

D = 2048
DH = 128
BLK = 128
R = 2
PLEN = 64
TOK_DEV = 512
PASS_DEV = 32
TOKENS = 2048
NPASS = 128
STORE_ROWS = 8192


def request_table(key):
    base = jax.random.fold_in(key, 11)
    owners_count = NPASS // PASS_DEV
    requests = TOK_DEV // BLK * R
    slot_most = max(1, 2 * requests // owners_count)
    slot_count = owners_count * slot_most
    subkeys = jax.random.split(base, 5)
    popular = jax.random.randint(subkeys[0], (owners_count,), 0, 2)
    hottest = jax.random.randint(subkeys[1], (), 0, owners_count)
    device = jnp.arange(owners_count, dtype=jnp.int32)[:, None]
    slot_ids = jnp.arange(slot_count, dtype=jnp.int32)[None, :]
    slot_owner = slot_ids // slot_most
    slot_rank = slot_ids % slot_most
    previous = (device - 1) % owners_count
    opposite = (device + owners_count // 2) % owners_count
    forced = ((slot_owner == hottest) | (slot_owner == previous)).astype(jnp.int32)
    halfway = ((slot_owner == opposite) & (slot_rank == 0)).astype(jnp.int32)
    leading = ((slot_owner == previous) & (slot_rank == 0)).astype(jnp.int32)
    tier = popular[slot_owner] + 3 * forced + 2 * halfway + 8 * leading
    noise = jax.random.randint(subkeys[2], (owners_count, slot_count), 0, 65536)
    score = (tier * 65536 + noise) * slot_count + slot_ids
    chosen = jnp.argsort(-score, axis=1)[:, :requests]
    chosen_owner = chosen // slot_most
    picks = jax.random.randint(subkeys[3], (owners_count, owners_count), 0, PASS_DEV)
    picks = picks.at[0, owners_count - 1].set(PASS_DEV - 1)
    picks = picks.at[1 % owners_count, 0].set(0)
    first_pick = jnp.take_along_axis(picks, chosen_owner, axis=1)
    local_ids = (first_pick + chosen % slot_most) % PASS_DEV
    passage = chosen_owner * PASS_DEV + local_ids
    shuffle = jax.random.randint(subkeys[4], (owners_count, requests), 0, 1 << 20) * requests
    shuffle = shuffle + jnp.arange(requests, dtype=jnp.int32)[None, :]
    arrangement = jnp.argsort(shuffle, axis=1)
    passage = jnp.take_along_axis(passage, arrangement, axis=1)
    return passage.reshape(-1, R).astype(jnp.int32)


def store_values(key):
    return jnp.clip(jax.random.normal(jax.random.fold_in(key, 21), (STORE_ROWS, D), jnp.float32), -5.0, 5.0)


def query_weight(key):
    fresh = jax.random.normal(jax.random.fold_in(key, 31), (D, D), jnp.float32)
    return jnp.clip(fresh, -6.0, 6.0) * D ** (-0.5)


def draw_passage_ids(key, part):
    return request_table(key)


def draw_store(key, part):
    return store_values(key).astype(jnp.bfloat16)


def draw_w_query(key, part):
    return query_weight(key).astype(jnp.bfloat16)


def draw_w_key(key, part):
    fresh = jnp.clip(jax.random.normal(jax.random.fold_in(key, 41), (D, D), jnp.float32), -6.0, 6.0) * D ** (-0.5)
    return fresh.astype(jnp.bfloat16)


def draw_normed(key, part):
    rows = jnp.clip(jax.random.normal(jax.random.fold_in(key, 51), (TOKENS, D), jnp.float32), -6.0, 6.0)
    return rows.astype(jnp.bfloat16)


def level_of(own_key, dims, pieces, low, largest):
    gain = 1.0
    for axis_at, parts in pieces:
        heights = jax.random.uniform(jax.random.fold_in(jax.random.fold_in(own_key, 6), axis_at), (parts,), jnp.float32, low / len(pieces), largest / len(pieces))
        gain = gain * jnp.repeat(jnp.exp(heights), dims[axis_at] // parts).reshape((-1,) + (1,) * (len(dims) - 1 - axis_at))
    return gain


def bell_draw(stream_key, dims, scale, bound, shards=(), kind=jnp.bfloat16):
    entries = jax.random.normal(stream_key, dims, jnp.float32) * scale
    if len(shards) > 0:
        entries = level_of(stream_key, dims, shards, -0.22, 0.18) * entries
    return jnp.clip(entries, min=-bound, max=bound).astype(kind)


def setup_inputs(seed: int = 0) -> dict:
    seeds = jax.random.split(jax.random.key(seed), 9)
    normed = draw_normed(jax.random.fold_in(seeds[8], 71), 0)
    store = draw_store(jax.random.fold_in(seeds[8], 71), 0)
    passage_ids = draw_passage_ids(jax.random.fold_in(seeds[8], 71), 0)
    w_query = draw_w_query(jax.random.fold_in(seeds[8], 71), 0)
    w_gate = bell_draw(seeds[4], (D, D), D ** -0.5, 0.125, ((1, 8),))
    w_key = draw_w_key(jax.random.fold_in(seeds[8], 71), 0)
    w_value = bell_draw(seeds[6], (D, D), D ** -0.5, 0.125, ((1, 8),))
    cotangent = bell_draw(seeds[7], (TOKENS, D), 1.0, 6.0, ((0, 4), (1, 8)))
    return dict(normed=normed, store=store, passage_ids=passage_ids, w_query=w_query, w_gate=w_gate, w_key=w_key, w_value=w_value, cotangent=cotangent)


def reference(normed, store, passage_ids, w_query, w_gate, w_key, w_value, cotangent):
    tokens, model_width = normed.shape
    blocks = tokens // BLK
    heads = model_width // DH
    score_scale = DH ** -0.5
    queries = jnp.dot(normed, w_query, preferred_element_type=jnp.float32).astype(jnp.bfloat16)
    gate_open = jax.nn.sigmoid(jnp.dot(normed, w_gate, preferred_element_type=jnp.float32))
    key_all = jnp.dot(store, w_key, preferred_element_type=jnp.float32).astype(jnp.bfloat16)
    value_all = jnp.dot(store, w_value, preferred_element_type=jnp.float32).astype(jnp.bfloat16)
    key_all = key_all.reshape(NPASS, PLEN, heads, DH)
    value_all = value_all.reshape(NPASS, PLEN, heads, DH)
    flat_ids = passage_ids.reshape(-1).astype(jnp.int32)
    key_rows = jnp.take(key_all, flat_ids, axis=0).reshape(blocks, R * PLEN, heads, DH).astype(jnp.float32)
    value_rows = jnp.take(value_all, flat_ids, axis=0).reshape(blocks, R * PLEN, heads, DH).astype(jnp.float32)
    q_blocks = queries.reshape(blocks, BLK, heads, DH).astype(jnp.float32)
    scores = jnp.einsum("bthd,bshd->bhts", q_blocks, key_rows) * score_scale
    attn_probs = jax.nn.softmax(scores, axis=-1)
    probs_low = attn_probs.astype(jnp.bfloat16).astype(jnp.float32)
    attended = jnp.einsum("bhts,bshd->bthd", probs_low, value_rows)
    gate_blocks = gate_open.reshape(blocks, BLK, heads, DH)
    upstream = cotangent.astype(jnp.float32).reshape(blocks, BLK, heads, DH)
    d_attended = (upstream * gate_blocks).astype(jnp.bfloat16).astype(jnp.float32)
    d_gate = (upstream * attended * gate_blocks * (1.0 - gate_blocks)).astype(jnp.bfloat16)
    d_values = jnp.einsum("bhts,bthd->bshd", probs_low, d_attended).astype(jnp.bfloat16)
    d_probs = jnp.einsum("bthd,bshd->bhts", d_attended, value_rows)
    row_delta = jnp.sum(d_probs * attn_probs, axis=-1, keepdims=True)
    d_scores = (attn_probs * (d_probs - row_delta) * score_scale).astype(jnp.bfloat16).astype(jnp.float32)
    d_query = jnp.einsum("bhts,bshd->bthd", d_scores, key_rows).astype(jnp.bfloat16).reshape(tokens, model_width)
    d_keys = jnp.einsum("bhts,bthd->bshd", d_scores, q_blocks).astype(jnp.bfloat16)
    grad_rows = jnp.dot(d_query, w_query.T, preferred_element_type=jnp.float32)
    grad_rows = grad_rows + jnp.dot(d_gate.reshape(tokens, model_width), w_gate.T, preferred_element_type=jnp.float32)
    reads_keys = d_keys.reshape(blocks * R, PLEN, model_width).astype(jnp.float32)
    reads_values = d_values.reshape(blocks * R, PLEN, model_width).astype(jnp.float32)
    summed_keys = jnp.zeros((NPASS, PLEN, model_width), jnp.float32).at[flat_ids].add(reads_keys)
    summed_values = jnp.zeros((NPASS, PLEN, model_width), jnp.float32).at[flat_ids].add(reads_values)
    grad_store = jnp.dot(summed_keys.reshape(NPASS * PLEN, model_width), w_key.astype(jnp.float32).T,
                         precision=lax.Precision.HIGHEST)
    grad_store = grad_store + jnp.dot(summed_values.reshape(NPASS * PLEN, model_width),
                                      w_value.astype(jnp.float32).T, precision=lax.Precision.HIGHEST)
    grad_query_weight = jnp.dot(normed.T, d_query, preferred_element_type=jnp.float32)
    return grad_rows, grad_store, grad_query_weight
```

```python
import functools

import jax
import jax.numpy as jnp
from jax import lax
from jax.experimental import pallas as pl
from jax.experimental.pallas import tpu as pltpu
from jax.sharding import PartitionSpec as P

DH = 128
BLK = 128
PLEN = 64
GROUP = 4
CORES = 2
F32 = jnp.float32
BF16 = jnp.bfloat16
MESH = pl.DeviceIdType.MESH


def dot_nn(a, b):
    return lax.dot_general(a, b, (((1,), (0,)), ((), ())), preferred_element_type=F32)


def dot_nt(a, b):
    return lax.dot_general(a, b, (((1,), (1,)), ((), ())), preferred_element_type=F32)


def dot_tn(a, b):
    return lax.dot_general(a, b, (((0,), (0,)), ((), ())), preferred_element_type=F32)


def rows_at(index, size):
    return pl.ds(pl.multiple_of(index * size, size), size)


def main_kernel(
    st_n, tp_n, reads, slots, pass_dev,
    ids, store_h, normed_h, w_q_h, w_g_h, w_k_h, w_v_h, cot_h,
    rows_out, ret_out, gqw_out, served_out,
    store, normed, w_q, w_g, w_k, w_v, cot, load_sem,
    mine, tables, req_of, slot_of, early_of, t_ss, t_rs,
    served, arr_e, arr_all, q_s, gate_s, dq_s, dg_s, dp_s,
    x_out, x_in, z_out, up_in, dn_in, own, part, r_out, r_in, g_out, g_in, g_own,
    kv_ss, kv_rs, x_ss, x_rs, z_ss, up_rs, dn_rs, r_ss, r_rs, g_ss, g_rs,
):
    me_st, me_tp = lax.axis_index("st"), lax.axis_index("tp")
    z_n = tp_n // CORES
    me_z, me_c = me_tp // CORES, me_tp % CORES
    mate = (me_st, me_z * CORES + 1 - me_c)
    tok, hw = cot.shape
    depth = w_q.shape[0]
    heads = hw // DH
    blocks = tok // BLK
    cw = depth // tp_n
    first = min(reads, slots)
    n_pos = blocks * reads
    scale = DH ** (-0.5)

    def st_peer(d):
        return lax.rem(me_st + d, st_n)

    def st_from(d):
        return lax.rem(me_st + st_n - d, st_n)

    def load(i, far, near):
        copy = pltpu.make_async_copy(far, near, load_sem.at[i])
        copy.start()
        return copy

    loads_a = [
        load(i, far, near)
        for i, (far, near) in enumerate(((w_k_h, w_k), (store_h, store), (w_v_h, w_v)))
    ]

    above, below = me_z < z_n - 1, me_z > 0
    barrier = pltpu.get_barrier_semaphore()

    def greet(device):
        pl.semaphore_signal(barrier, inc=1, device_id=device, device_id_type=MESH)

    for d in range(1, st_n):
        greet((st_peer(d), me_tp))

    @pl.when(above)
    def _():
        greet((me_st, (me_z + 1) * CORES + me_c))

    @pl.when(below)
    def _():
        greet((me_st, (me_z - 1) * CORES + me_c))

    greet(mate)

    passages = [ids[i % reads, i // reads] for i in range(n_pos)]
    owners = [lax.div(p, jnp.int32(pass_dev)) for p in passages]
    ranks = []
    for i in range(n_pos):
        rank = jnp.int32(0)
        for j in range(i):
            rank = rank + jnp.where(owners[j] == owners[i], 1, 0)
        ranks.append(rank)
    places = [owners[i] * slots + ranks[i] for i in range(n_pos)]
    for i in range(n_pos):
        slot_of[i] = places[i]
        early_of[i] = owners[i] * first + jnp.minimum(ranks[i], first - 1)
    for s in range(st_n * slots):
        local, position = jnp.int32(-1), jnp.int32(0)
        for i in range(n_pos):
            hit = places[i] == s
            local = jnp.where(hit, passages[i] - (s // slots) * pass_dev, local)
            position = jnp.where(hit, i, position)
        mine[s] = local
        req_of[s] = position

    pl.semaphore_wait(
        barrier, st_n + jnp.where(above, 1, 0) + jnp.where(below, 1, 0)
    )

    def remote(src, dst, ss, rs, dev):
        return pltpu.make_async_remote_copy(
            src_ref=src, dst_ref=dst, send_sem=ss, recv_sem=rs, device_id=dev, device_id_type=MESH
        )

    sends = []

    def go(copy):
        copy.start()
        sends.append(copy)

    for d in range(1, st_n):
        go(remote(mine, tables.at[d], t_ss.at[d], t_rs.at[d], (st_peer(d), me_tp)))
    loads_b = [
        load(3 + i, far, near)
        for i, (far, near) in enumerate(
            ((normed_h, normed), (w_q_h, w_q), (w_g_h, w_g), (cot_h, cot))
        )
    ]
    for copy in loads_a:
        copy.wait()
    for d in range(1, st_n):
        remote(tables.at[d], tables.at[d], t_ss.at[d], t_rs.at[d], (st_peer(d), me_tp)).wait_recv()

    def wanted(d, k):
        at = me_st * slots + k
        return tables[st_n - d, at] if d else mine[at]

    dists = list(range(1, st_n)) + [0]

    def kv_copy(d, k, outgoing):
        owner = me_st if outgoing else st_from(d)
        landing = arr_e.at[owner * first + k] if k < first else arr_all.at[owner * slots + k]
        n = d * slots + k
        source = served.at[n] if outgoing else landing
        return remote(source, landing, kv_ss.at[n], kv_rs.at[n], (st_peer(d), me_tp))

    def project(k, some):
        rows = jnp.concatenate(
            [store[jnp.maximum(wanted(d, k), 0)] for d in some], axis=0
        )
        keys = dot_nn(rows, w_k[...]).astype(BF16)
        values = dot_nn(rows, w_v[...]).astype(BF16)
        for i, d in enumerate(some):
            span = slice(i * PLEN, (i + 1) * PLEN)
            if d:
                served[d * slots + k, :, :hw] = keys[span]
                served[d * slots + k, :, hw:] = values[span]
                go(kv_copy(d, k, True))
            elif k < first:
                arr_e[me_st * first + k, :, :hw] = keys[span]
                arr_e[me_st * first + k, :, hw:] = values[span]
            else:
                arr_all[me_st * slots + k, :, :hw] = keys[span]
                arr_all[me_st * slots + k, :, hw:] = values[span]

    for k in range(slots):
        for i in range(0, st_n, GROUP):
            project(k, dists[i:i + GROUP])

    for d in range(st_n):
        for k in range(slots):
            served_out[st_peer(d) * slots + k] = wanted(d, k)

    for copy in loads_b:
        copy.wait()
    tile = 2 * BLK

    @pl.loop(0, tok // tile)
    def _(i):
        span = rows_at(i, tile)
        q_s[span, :] = dot_nn(normed[span, :], w_q[...]).astype(BF16)
        gate_s[span, :] = jax.nn.sigmoid(dot_nn(normed[span, :], w_g[...]))

    def kv_arrived(ranks):
        for k in ranks:
            for d in range(1, st_n):
                kv_copy(d, k, False).wait_recv()

    span = reads * PLEN

    def attend(b):
        if b == 0 or slots == first:
            parts = [arr_e[early_of[b * reads + r]] for r in range(reads)]
        else:
            parts = [arr_all[slot_of[b * reads + r]] for r in range(reads)]
        kv = jnp.concatenate(parts, axis=0)
        toks = slice(b * BLK, (b + 1) * BLK)
        ctx = slice(b * span, (b + 1) * span)
        for h in range(heads):
            ch = slice(h * DH, (h + 1) * DH)
            chv = slice(hw + h * DH, hw + (h + 1) * DH)
            k, v = kv[:, ch], kv[:, chv]
            q = q_s[toks, ch]
            gate = gate_s[toks, ch]
            up = cot[toks, ch].astype(F32)
            d_att = (up * gate).astype(BF16)
            d_p = dot_nt(d_att, v)
            s = dot_nt(q, k) * scale
            e = jnp.exp(s - jnp.max(s, axis=1, keepdims=True))
            p = e / jnp.sum(e, axis=1, keepdims=True)
            low = p.astype(BF16)
            att = dot_nn(low, v)
            dg_s[toks, ch] = (up * att * gate * (1.0 - gate)).astype(BF16)
            dp_s[ctx, chv] = dot_tn(low, d_att).astype(BF16)
            delta = jnp.sum(d_p * p, axis=1, keepdims=True)
            d_s = (p * (d_p - delta) * scale).astype(BF16)
            dq_s[toks, ch] = dot_nn(d_s, k).astype(BF16)
            dp_s[ctx, ch] = dot_tn(d_s, q).astype(BF16)

    def chunk(g, t):
        which, b = g
        w_rows = rows_at(t, cw)
        if which == 0:
            ctx = slice(b * span, (b + 1) * span)
            return dot_nt(dp_s[ctx, :hw], w_k[w_rows, :]) + dot_nt(dp_s[ctx, hw:], w_v[w_rows, :])
        toks = slice(b * BLK, (b + 1) * BLK)
        return dot_nt(dq_s[toks, :], w_q[w_rows, :]) + dot_nt(dg_s[toks, :], w_g[w_rows, :])

    order = []
    for i in range((z_n + 1) // 2):
        order += [z_n - 1 - i, i] if z_n - 1 - i != i else [i]

    def piece_of(g, t):
        return (g[0] * blocks + g[1]) * z_n + t

    def mate_copy(n):
        return remote(x_out.at[n], x_in.at[n], x_ss.at[n], x_rs.at[n], mate)

    def hop(n, up):
        landing, rs = (up_in, up_rs) if up else (dn_in, dn_rs)
        to = me_z + 1 if up else me_z - 1
        return remote(
            z_out.at[n], landing.at[n], z_ss.at[n], rs.at[n], (me_st, to * CORES + me_c)
        )

    def give(g):
        for t in order:
            n = piece_of(g, t)
            x_out[n] = chunk(g, t * CORES + 1 - me_c).astype(BF16)
            go(mate_copy(n))

    def take(g):
        for t in order:
            n = piece_of(g, t)
            own[n] = chunk(g, t * CORES + me_c)
        for t in order:
            n = piece_of(g, t)
            mate_copy(n).wait_recv()
            total = own[n] + x_in[n].astype(F32)
            own[n] = total

            @pl.when(jnp.logical_and(me_z == 0, t > me_z))
            def _():
                z_out[n] = total.astype(BF16)
                hop(n, True).start()

            @pl.when(jnp.logical_and(me_z == z_n - 1, t < me_z))
            def _():
                z_out[n] = total.astype(BF16)
                hop(n, False).start()

    def relay(g, k):
        @pl.when(me_z == k)
        def _():
            for t in range(z_n - 1, k, -1):
                n = piece_of(g, t)
                hop(n, True).wait_recv()
                z_out[n] = (own[n] + up_in[n].astype(F32)).astype(BF16)
                hop(n, True).start()

        @pl.when(me_z == z_n - 1 - k)
        def _():
            for t in range(z_n - 1 - k):
                n = piece_of(g, t)
                hop(n, False).wait_recv()
                z_out[n] = (own[n] + dn_in[n].astype(F32)).astype(BF16)
                hop(n, False).start()

    def gathered(g):
        n = piece_of(g, me_z)

        @pl.when(below)
        def _():
            hop(n, True).wait_recv()
            own[n] = own[n] + up_in[n].astype(F32)

        @pl.when(above)
        def _():
            hop(n, False).wait_recv()
            own[n] = own[n] + dn_in[n].astype(F32)

        which, b = g
        if which == 0:
            part[b * reads:(b + 1) * reads] = own[n].astype(BF16).reshape(reads, PLEN, cw)
        else:
            rows_out[b * BLK:(b + 1) * BLK, :] = own[n]

    kv_arrived(range(first))
    attend(0)
    groups = [(0, 0), (1, 0)] + [(0, b) for b in range(1, blocks)] + [(1, b) for b in range(1, blocks)]
    give(groups[0])
    give(groups[1])
    take(groups[0])
    take(groups[1])
    if slots > first:
        for o in range(st_n):
            for k in range(first):
                arr_all[o * slots + k] = arr_e[o * first + k]
        kv_arrived(range(first, slots))

    steps = len(groups) + max(z_n - 2, 0)
    relayed = [0]

    def relay_step():
        j = relayed[0]
        relayed[0] += 1
        for k in range(1, z_n - 1):
            if 0 <= j - (k - 1) < len(groups):
                relay(groups[j - (k - 1)], k)

    for b in range(1, blocks):
        attend(b)
        give((0, b))
        if b > 1:
            take((0, b - 1))
        if b == 2:
            relay_step()
    for b in range(1, blocks):
        give((1, b))
        if b == 1:
            take((0, blocks - 1))
            relay_step()
        else:
            take((1, b - 1))
    take((1, blocks - 1))
    relay_step()

    dw = depth // st_n
    for d in list(range(1, st_n)) + [0]:
        term = dot_tn(normed[:, rows_at(st_peer(d), dw)], dq_s[...])
        if d == 0:
            g_own[...] = term
        else:
            g_out[d] = term.astype(BF16)
            go(remote(
                g_out.at[d], g_in.at[d], g_ss.at[d], g_rs.at[d], (st_peer(d), me_tp)
            ))

    reads_done = max(i for i, g in enumerate(groups) if g[0] == 0) + max(z_n - 2, 1)
    while relayed[0] < min(reads_done, steps):
        relay_step()
    for b in range(blocks):
        gathered((0, b))
    for s in range(st_n * slots):
        r_out[s] = part[req_of[s]]
    for d in range(1, st_n):
        go(remote(
            r_out.at[rows_at(st_peer(d), slots)], r_in.at[rows_at(me_st, slots)],
            r_ss.at[d], r_rs.at[d], (st_peer(d), me_tp),
        ))
    ret_out[rows_at(me_st, slots)] = r_out[rows_at(me_st, slots)]

    while relayed[0] < steps - 1:
        relay_step()

    total = g_own[...]
    for d in range(1, st_n):
        remote(g_in.at[d], g_in.at[d], g_ss.at[d], g_rs.at[d], (st_peer(d), me_tp)).wait_recv()
        total = total + g_in[d].astype(F32)
    gqw_out[...] = total
    while relayed[0] < steps:
        relay_step()

    for d in range(1, st_n):
        here = rows_at(st_from(d), slots)
        remote(
            r_in.at[here], r_in.at[here], r_ss.at[d], r_rs.at[d], (st_peer(d), me_tp)
        ).wait_recv()
        ret_out[here] = r_in[here]

    for b in range(blocks):
        gathered((1, b))
    for copy in sends:
        copy.wait_send()
    for g in groups:
        for t in range(z_n):

            @pl.when(t != me_z)
            def _():
                hop(piece_of(g, t), True).wait_send()


def main_call(st_n, tp_n, ids, store, normed, w_q, w_g, w_k, w_v, cot):
    reads, blocks = ids.shape
    tok, hw = cot.shape
    depth = w_q.shape[0]
    cw, dw, z_n = depth // tp_n, depth // st_n, tp_n // CORES
    pass_dev = store.shape[0]
    n_pos = blocks * reads
    slots = max(1, 2 * n_pos // st_n)
    first = min(reads, slots)
    ctx = blocks * reads * PLEN
    slot_total = st_n * slots
    vmem = pl.BlockSpec(memory_space=pltpu.VMEM)
    smem = pl.BlockSpec(memory_space=pltpu.SMEM)
    pieces = 2 * blocks * z_n
    piece = lambda kind=BF16: pltpu.VMEM((pieces, BLK, cw), kind)
    sem = lambda n: pltpu.SemaphoreType.DMA((n,))
    table = lambda *n: pltpu.SMEM(n, jnp.int32)
    assert ctx == tok
    return pl.pallas_call(
        functools.partial(main_kernel, st_n, tp_n, reads, slots, pass_dev),
        out_shape=(
            jax.ShapeDtypeStruct((tok, cw), F32),
            jax.ShapeDtypeStruct((slot_total, PLEN, cw), BF16),
            jax.ShapeDtypeStruct((dw, hw), F32),
            jax.ShapeDtypeStruct((slot_total,), jnp.int32),
        ),
        in_specs=[smem] + [pl.BlockSpec(memory_space=pl.ANY)] * 7,
        out_specs=(vmem, vmem, vmem, smem),
        scratch_shapes=[
            *[pltpu.VMEM(a.shape, a.dtype) for a in (store, normed, w_q, w_g, w_k, w_v, cot)],
            sem(7),
            table(slot_total), table(st_n, slot_total), table(slot_total), table(n_pos), table(n_pos),
            sem(st_n), sem(st_n),
            pltpu.VMEM((slot_total, PLEN, 2 * hw), BF16),
            pltpu.VMEM((st_n * first, PLEN, 2 * hw), BF16),
            pltpu.VMEM((slot_total, PLEN, 2 * hw), BF16),
            pltpu.VMEM((tok, hw), BF16),
            pltpu.VMEM((tok, hw), F32),
            pltpu.VMEM((tok, hw), BF16),
            pltpu.VMEM((tok, hw), BF16),
            pltpu.VMEM((ctx, 2 * hw), BF16),
            piece(), piece(), piece(), piece(), piece(), piece(F32),
            pltpu.VMEM((ctx // PLEN, PLEN, cw), BF16),
            pltpu.VMEM((slot_total, PLEN, cw), BF16),
            pltpu.VMEM((slot_total, PLEN, cw), BF16),
            pltpu.VMEM((st_n, dw, hw), BF16),
            pltpu.VMEM((st_n, dw, hw), BF16),
            pltpu.VMEM((dw, hw), F32),
            sem(slot_total), sem(slot_total),
            sem(pieces), sem(pieces), sem(pieces), sem(pieces), sem(pieces),
            sem(st_n), sem(st_n), sem(st_n), sem(st_n),
        ],
        compiler_params=pltpu.CompilerParams(
            collective_id=0, has_side_effects=True, vmem_limit_bytes=56 << 20
        ),
        name="main",
    )(ids, store, normed, w_q, w_g, w_k, w_v, cot)


def spread_kernel(ids, returned, rows, gqw, out_ref, rows_ref, gqw_ref):
    rows_ref[...] = rows[...]
    gqw_ref[...] = gqw[...]
    out_ref[...] = jnp.zeros_like(out_ref)
    for s in range(ids.shape[0]):
        passage = ids[s]

        @pl.when(passage >= 0)
        def _():
            span = rows_at(passage, PLEN)
            out_ref[span, :] += returned[s].astype(F32)


def spread(ids, returned, grad_rows, grad_query_weight, rows):
    vmem = pl.BlockSpec(memory_space=pltpu.VMEM)
    return pl.pallas_call(
        spread_kernel,
        out_shape=(
            jax.ShapeDtypeStruct((rows, returned.shape[2]), F32),
            jax.ShapeDtypeStruct(grad_rows.shape, F32),
            jax.ShapeDtypeStruct(grad_query_weight.shape, F32),
        ),
        in_specs=[pl.BlockSpec(memory_space=pltpu.SMEM), vmem, vmem, vmem],
        out_specs=(vmem, vmem, vmem),
        compiler_params=pltpu.CompilerParams(vmem_limit_bytes=60 << 20),
        name="spread",
    )(ids, returned, grad_rows, grad_query_weight)


def shards(normed, store, passage_ids, w_query, w_gate, w_key, w_value, cotangent):
    grad_rows, returned, grad_query_weight, served_ids = main_call(
        lax.axis_size("st"), lax.axis_size("tp"), passage_ids.T,
        store.reshape(-1, PLEN, store.shape[1]), normed, w_query, w_gate, w_key, w_value, cotangent,
    )
    grad_store, grad_rows, grad_query_weight = spread(
        served_ids, returned, grad_rows, grad_query_weight, store.shape[0]
    )
    return (grad_rows, grad_store, grad_query_weight)


def solution(mesh):
    placed = (
        P("st", None),
        P("st", None),
        P("st", None),
        P(None, "tp"),
        P(None, "tp"),
        P(None, "tp"),
        P(None, "tp"),
        P("st", "tp"),
    )
    return jax.shard_map(
        shards,
        mesh=mesh,
        in_specs=placed,
        out_specs=(P("st", "tp"), P("st", "tp"), P("st", "tp")),
        check_vma=False,
    )
```

```python
import functools

import jax
import jax.numpy as jnp
from jax import lax
from jax.experimental import pallas as pl
from jax.experimental.pallas import tpu as pltpu
from jax.sharding import PartitionSpec as P

DH = 128
BLK = 128
PLEN = 64
GROUP = 4
CORES = 2
F32 = jnp.float32
BF16 = jnp.bfloat16
MESH = pl.DeviceIdType.MESH


def dot_nn(a, b):
    return lax.dot_general(a, b, (((1,), (0,)), ((), ())), preferred_element_type=F32)


def dot_nt(a, b):
    return lax.dot_general(a, b, (((1,), (1,)), ((), ())), preferred_element_type=F32)


def dot_tn(a, b):
    return lax.dot_general(a, b, (((0,), (0,)), ((), ())), preferred_element_type=F32)


def rows_at(index, size):
    return pl.ds(pl.multiple_of(index * size, size), size)


def main_kernel(
    st_n, tp_n, reads, slots, pass_dev,
    ids, store_h, normed_h, w_q_h, w_g_h, w_k_h, w_v_h, cot_h,
    rows_out, ret_out, gqw_out, served_out,
    store, normed, w_q, w_g, w_k, w_v, cot, load_sem,
    mine, tables, served_ids, req_of, slot_of, early_of, t_ss, t_rs,
    served, arr_e, arr_all, q_s, gate_s, dq_s, dg_s, dp_s,
    x_out, x_in, z_out, up_in, dn_in, own, part, r_out, r_in, g_out, g_in, g_own,
    kv_ss, kv_rs, x_ss, x_rs, z_ss, z_rs, r_ss, r_rs, g_ss, g_rs, out_sem,
):
    me_st, me_tp = lax.axis_index("st"), lax.axis_index("tp")
    z_n = tp_n // CORES
    me_z, me_c = me_tp // CORES, me_tp % CORES
    mate = (me_st, me_z * CORES + 1 - me_c)
    tok, hw = cot.shape
    depth = w_q.shape[0]
    heads = hw // DH
    blocks = tok // BLK
    cw = depth // tp_n
    first = min(reads, slots)
    n_pos = blocks * reads
    scale = DH ** (-0.5)

    def st_peer(d):
        return lax.rem(me_st + d, st_n)

    def st_from(d):
        return lax.rem(me_st + st_n - d, st_n)

    def load(i, far, near):
        copy = pltpu.make_async_copy(far, near, load_sem.at[i])
        copy.start()
        return copy

    loads_a = [
        load(i, far, near)
        for i, (far, near) in enumerate(((w_k_h, w_k), (store_h, store), (w_v_h, w_v)))
    ]

    above, below = me_z < z_n - 1, me_z > 0
    barrier = pltpu.get_barrier_semaphore()

    def greet(device):
        pl.semaphore_signal(barrier, inc=1, device_id=device, device_id_type=MESH)

    for d in range(1, st_n):
        for c in range(CORES):
            greet((st_peer(d), me_z * CORES + c))

    @pl.when(above)
    def _():
        greet((me_st, (me_z + 1) * CORES + me_c))

    @pl.when(below)
    def _():
        greet((me_st, (me_z - 1) * CORES + me_c))

    greet(mate)

    passages = [ids[i % reads, i // reads] for i in range(n_pos)]
    owners = [lax.div(p, jnp.int32(pass_dev)) for p in passages]
    ranks = []
    for i in range(n_pos):
        rank = jnp.int32(0)
        for j in range(i):
            rank = rank + jnp.where(owners[j] == owners[i], 1, 0)
        ranks.append(rank)
    places = [owners[i] * slots + ranks[i] for i in range(n_pos)]
    for i in range(n_pos):
        slot_of[i] = places[i]
        early_of[i] = owners[i] * first + jnp.minimum(ranks[i], first - 1)
    for s in range(st_n * slots):
        local, position = jnp.int32(-1), jnp.int32(0)
        for i in range(n_pos):
            hit = places[i] == s
            local = jnp.where(hit, passages[i] - (s // slots) * pass_dev, local)
            position = jnp.where(hit, i, position)
        mine[s] = local
        req_of[s] = position

    def barrier_wait():
        pl.semaphore_wait(
            barrier, CORES * (st_n - 1) + 1 + jnp.where(above, 1, 0) + jnp.where(below, 1, 0)
        )

    barrier_wait()

    def remote(src, dst, ss, rs, dev):
        return pltpu.make_async_remote_copy(
            src_ref=src, dst_ref=dst, send_sem=ss, recv_sem=rs, device_id=dev, device_id_type=MESH
        )

    def landed(ref, rs):
        remote(ref, ref, out_sem.at[0], rs, mate).wait_recv()

    def gone(ref, ss):
        remote(ref, ref, ss, out_sem.at[0], mate).wait_send()

    def table_copy(d, c):
        return remote(
            mine, tables.at[d], t_ss.at[c], t_rs.at[0], (st_peer(d), me_z * CORES + c)
        )

    @pl.when(me_c == CORES - 1)
    def _():
        for c in range(CORES):
            for d in range(1, st_n):
                table_copy(d, c).start()

    loads_b = [
        load(3 + i, far, near)
        for i, (far, near) in enumerate(
            ((normed_h, normed), (w_q_h, w_q), (w_g_h, w_g), (cot_h, cot))
        )
    ]

    def store_wait():
        for copy in loads_a:
            copy.wait()

    def table_wait():
        landed(tables.at[:st_n - 1], t_rs.at[0])

    store_wait()
    table_wait()

    def wanted(d, k):
        at = me_st * slots + k
        return tables[st_n - d, at] if d else mine[at]

    dists = list(range(1, st_n)) + [0]
    halves = (0, 1)

    def kv_copy(d, k):
        landing = arr_e.at[me_st * first + k] if k < first else arr_all.at[me_st * slots + k]
        source = served.at[d * slots + k]
        late = 0 if k < first else 1
        return remote(source, landing, kv_ss.at[late], kv_rs.at[late], (st_peer(d), me_tp))

    def project(k, some):
        rows = jnp.concatenate([store[jnp.maximum(wanted(d, k), 0)] for d in some], axis=0)
        for half in halves:
            made = dot_nn(rows, (w_k, w_v)[half][...]).astype(BF16)
            for i, d in enumerate(some):
                piece = made[i * PLEN:(i + 1) * PLEN]
                if d:
                    served[d * slots + k, half] = piece
                elif k < first:
                    arr_e[me_st * first + k, half] = piece
                else:
                    arr_all[me_st * slots + k, half] = piece
        if k < first:
            for d in some:
                if d:
                    kv_copy(d, k).start()

    for k in range(slots):
        for i in range(0, st_n, GROUP):
            project(k, dists[i:i + GROUP])

    for d in range(st_n):
        for k in range(slots):
            served_ids[st_peer(d) * slots + k] = wanted(d, k)

    outs = []

    def put(i, near, far):
        copy = pltpu.make_async_copy(near, far, out_sem.at[i])
        copy.start()
        outs.append(copy)

    put(2, served_ids, served_out)
    for copy in loads_b:
        copy.wait()
    tile = 2 * BLK

    @pl.loop(0, tok // tile)
    def _(i):
        span = rows_at(i, tile)
        q_s[span, :] = dot_nn(normed[span, :], w_q[...]).astype(BF16)
        gate_s[span, :] = jax.nn.sigmoid(dot_nn(normed[span, :], w_g[...]))

    late = (st_n - 1) * (slots - first)

    def kv_arrived(phase):
        if phase == 0:
            landed(arr_e.at[:(st_n - 1) * first], kv_rs.at[0])
        else:
            landed(arr_all.at[:late], kv_rs.at[1])

    span = reads * PLEN

    def attend(b):
        if b == 0 or slots == first:
            parts = [arr_e[early_of[b * reads + r]] for r in range(reads)]
        else:
            parts = [arr_all[slot_of[b * reads + r]] for r in range(reads)]
        keys = jnp.concatenate([part[0] for part in parts], axis=0)
        values = jnp.concatenate([part[1] for part in parts], axis=0)
        toks = slice(b * BLK, (b + 1) * BLK)
        ctx = slice(b * span, (b + 1) * span)
        for h in range(heads):
            ch = slice(h * DH, (h + 1) * DH)
            chv = slice(hw + h * DH, hw + (h + 1) * DH)
            k, v = keys[:, ch], values[:, ch]
            q = q_s[toks, ch]
            gate = gate_s[toks, ch]
            up = cot[toks, ch].astype(F32)
            d_att = (up * gate).astype(BF16)
            d_p = dot_nt(d_att, v)
            s = dot_nt(q, k) * scale
            e = jnp.exp(s - jnp.max(s, axis=1, keepdims=True))
            p = e / jnp.sum(e, axis=1, keepdims=True)
            low = p.astype(BF16)
            att = dot_nn(low, v)
            dg_s[toks, ch] = (up * att * gate * (1.0 - gate)).astype(BF16)
            dp_s[ctx, chv] = dot_tn(low, d_att).astype(BF16)
            delta = jnp.sum(d_p * p, axis=1, keepdims=True)
            d_s = (p * (d_p - delta) * scale).astype(BF16)
            dq_s[toks, ch] = dot_nn(d_s, k).astype(BF16)
            dp_s[ctx, ch] = dot_tn(d_s, q).astype(BF16)

    def chunk(g, t):
        which, b = g
        w_rows = rows_at(t, cw)
        if which == 0:
            ctx = slice(b * span, (b + 1) * span)
            return dot_nt(dp_s[ctx, :hw], w_k[w_rows, :]) + dot_nt(dp_s[ctx, hw:], w_v[w_rows, :])
        toks = slice(b * BLK, (b + 1) * BLK)
        return dot_nt(dq_s[toks, :], w_q[w_rows, :]) + dot_nt(dg_s[toks, :], w_g[w_rows, :])

    order = []
    for i in range((z_n + 1) // 2):
        order += [z_n - 1 - i, i] if z_n - 1 - i != i else [i]

    def piece_of(g, t):
        return (g[0] * blocks + g[1]) * z_n + t

    def all_of(g):
        at = piece_of(g, 0)
        return slice(at, at + z_n)

    batches = [[(0, 0)], [(1, 0)]] + [[(0, b)] for b in range(1, blocks)]
    batches.append([(1, b) for b in range(1, blocks)])
    early_groups = [g for batch in batches[:-1] for g in batch]

    def hop(g, t, up):
        n = piece_of(g, t)
        to = me_z + 1 if up else me_z - 1
        return remote(
            z_out.at[n], (up_in if up else dn_in).at[n],
            z_ss.at[0 if g in early_groups else 1],
            z_rs.at[piece_of(g, 0) // z_n * (z_n + 1) + t + (1 if up else 0)],
            (me_st, to * CORES + me_c),
        )

    def give(g):
        for t in order:
            x_out[piece_of(g, t)] = chunk(g, t * CORES + 1 - me_c).astype(BF16)
        i = piece_of(g, 0) // z_n
        for t in order:
            n = piece_of(g, t)
            remote(x_out.at[n], x_in.at[n], x_ss.at[i], x_rs.at[i], mate).start()

    def take(g):
        for t in order:
            own[piece_of(g, t)] = chunk(g, t * CORES + me_c)
        landed(x_in.at[all_of(g)], x_rs.at[piece_of(g, 0) // z_n])
        for t in order:
            n = piece_of(g, t)
            own[n] = own[n] + x_in[n].astype(F32)

    def depart(batch):
        @pl.when(me_z == 0)
        def _():
            for t in range(z_n - 1, 0, -1):
                for g in batch:
                    n = piece_of(g, t)
                    z_out[n] = own[n].astype(BF16)
                    hop(g, t, True).start()

        @pl.when(me_z == z_n - 1)
        def _():
            for t in range(z_n - 1):
                for g in batch:
                    n = piece_of(g, t)
                    z_out[n] = own[n].astype(BF16)
                    hop(g, t, False).start()

    def pass_on(batch, up, t):
        landing = up_in if up else dn_in
        for g in batch:
            n = piece_of(g, t)
            hop(g, t, up).wait_recv()
            z_out[n] = (own[n] + landing[n].astype(F32)).astype(BF16)
            hop(g, t, up).start()

    def relay(batch, z, stages):
        moves = [(z_n - 1 - t, z, True, t) for t in range(z + 1, z_n)]
        moves += [(t, z_n - 1 - z, False, t) for t in range(z)]
        moves = [m for m in moves if m[1] in stages]

        @pl.when(me_z == z)
        def _():
            for m in sorted(moves, key=lambda m: (m[0] + m[1], -m[1])):
                pass_on(batch, m[2], m[3])

    def gathered(g):
        n = piece_of(g, me_z)

        @pl.when(below)
        def _():
            hop(g, me_z, True).wait_recv()
            own[n] = own[n] + up_in[n].astype(F32)

        @pl.when(above)
        def _():
            hop(g, me_z, False).wait_recv()
            own[n] = own[n] + dn_in[n].astype(F32)

        which, b = g
        if which == 0:
            part[b * reads:(b + 1) * reads] = own[n].astype(BF16).reshape(reads, PLEN, cw)

    reads_end = blocks
    relayed = [0]

    def relay_step():
        j = relayed[0]
        relayed[0] += 1
        for z in range(1, z_n - 1):
            for k in range(1, z_n - 1):
                if 0 <= j - (k - 1) <= reads_end and k in (z, z_n - 1 - z):
                    relay(batches[j - (k - 1)], z, (k,))

    kv_arrived(0)
    for k in range(first, slots):
        for d in range(1, st_n):
            kv_copy(d, k).start()
    attend(0)
    give((0, 0))
    take((0, 0))
    depart(batches[0])
    give((1, 0))
    take((1, 0))
    depart(batches[1])
    if slots > first:
        for o in range(st_n):
            for k in range(first):
                arr_all[o * slots + k] = arr_e[o * first + k]
        kv_arrived(1)

    for b in range(1, blocks):
        attend(b)
        give((0, b))
        if b > 1:
            take((0, b - 1))
            depart([(0, b - 1)])
        if b == 2:
            relay_step()
    for b in range(1, blocks):
        give((1, b))
        if b == 1:
            take((0, blocks - 1))
            depart([(0, blocks - 1)])
            relay_step()
        else:
            take((1, b - 1))
    take((1, blocks - 1))
    depart(batches[-1])
    relay_step()

    dw = depth // st_n
    for d in list(range(1, st_n)) + [0]:
        term = dot_tn(normed[:, rows_at(st_peer(d), dw)], dq_s[...])
        if d == 0:
            g_own[...] = term
        else:
            g_out[d] = term.astype(BF16)
            remote(
                g_out.at[d], g_in.at[d], g_ss.at[0], g_rs.at[0], (st_peer(d), me_tp)
            ).start()

    while relayed[0] < reads_end + 1 + max(z_n - 3, 0):
        relay_step()
    for b in range(blocks):
        gathered((0, b))
    for s in range(st_n * slots):
        r_out[s] = part[req_of[s]]
    for d in range(1, st_n):
        remote(
            r_out.at[rows_at(st_peer(d), slots)], r_in.at[rows_at(me_st, slots)],
            r_ss.at[0], r_rs.at[0], (st_peer(d), me_tp),
        ).start()
    r_in[rows_at(me_st, slots)] = r_out[rows_at(me_st, slots)]

    def gqw_wait():
        total = g_own[...]
        landed(g_in.at[:st_n - 1], g_rs.at[0])
        for d in range(1, st_n):
            total = total + g_in[d].astype(F32)
        g_own[...] = total
        put(1, g_own, gqw_out)

    def send_wait():
        gone(served.at[:(st_n - 1) * first], kv_ss.at[0])
        if slots > first:
            gone(served.at[:late], kv_ss.at[1])
        for g in [g for batch in batches for g in batch]:
            gone(x_out.at[all_of(g)], x_ss.at[piece_of(g, 0) // z_n])
        gone(g_out.at[:st_n - 1], g_ss.at[0])
        gone(z_out.at[:len(early_groups) * (z_n - 1)], z_ss.at[0])

    @pl.when(me_c == CORES - 1)
    def _():
        for c in range(CORES):
            gone(tables.at[:st_n - 1], t_ss.at[c])

    for z in range(1, z_n - 1):
        relay(batches[-1], z, range(z_n))
    gqw_wait()
    send_wait()

    def ret_wait():
        landed(r_in.at[:(st_n - 1) * slots], r_rs.at[0])
        put(0, r_in, ret_out)

    ret_wait()
    for b in range(blocks):
        gathered((1, b))
        put(3 + b, own.at[piece_of((1, b), me_z)], rows_out.at[b * BLK:(b + 1) * BLK])
    gone(z_out.at[:len(batches[-1]) * (z_n - 1)], z_ss.at[1])
    gone(r_out.at[:(st_n - 1) * slots], r_ss.at[0])

    def out_wait():
        for copy in outs:
            copy.wait()

    out_wait()


def main_call(st_n, tp_n, ids, store, normed, w_q, w_g, w_k, w_v, cot):
    reads, blocks = ids.shape
    tok, hw = cot.shape
    depth = w_q.shape[0]
    cw, dw, z_n = depth // tp_n, depth // st_n, tp_n // CORES
    pass_dev = store.shape[0]
    n_pos = blocks * reads
    slots = max(1, 2 * n_pos // st_n)
    first = min(reads, slots)
    ctx = blocks * reads * PLEN
    slot_total = st_n * slots
    hbm = pl.BlockSpec(memory_space=pl.ANY)
    smem = pl.BlockSpec(memory_space=pltpu.SMEM)
    pieces = 2 * blocks * z_n
    piece = lambda kind=BF16: pltpu.VMEM((pieces, BLK, cw), kind)
    sem = lambda n: pltpu.SemaphoreType.DMA((n,))
    table = lambda *n: pltpu.SMEM(n, jnp.int32)
    assert ctx == tok
    return pl.pallas_call(
        functools.partial(main_kernel, st_n, tp_n, reads, slots, pass_dev),
        out_shape=(
            jax.ShapeDtypeStruct((tok, cw), F32),
            jax.ShapeDtypeStruct((slot_total, PLEN, cw), BF16),
            jax.ShapeDtypeStruct((dw, hw), F32),
            jax.ShapeDtypeStruct((slot_total,), jnp.int32),
        ),
        in_specs=[smem] + [hbm] * 7,
        out_specs=(hbm, hbm, hbm, hbm),
        scratch_shapes=[
            *[pltpu.VMEM(a.shape, a.dtype) for a in (store, normed, w_q, w_g, w_k, w_v, cot)],
            sem(7),
            table(slot_total), table(st_n, slot_total), table(slot_total),
            table(slot_total), table(n_pos), table(n_pos),
            sem(CORES), sem(1),
            pltpu.VMEM((slot_total, 2, PLEN, hw), BF16),
            pltpu.VMEM((st_n * first, 2, PLEN, hw), BF16),
            pltpu.VMEM((slot_total, 2, PLEN, hw), BF16),
            pltpu.VMEM((tok, hw), BF16),
            pltpu.VMEM((tok, hw), F32),
            pltpu.VMEM((tok, hw), BF16),
            pltpu.VMEM((tok, hw), BF16),
            pltpu.VMEM((ctx, 2 * hw), BF16),
            piece(), piece(), piece(), piece(), piece(), piece(F32),
            pltpu.VMEM((ctx // PLEN, PLEN, cw), BF16),
            pltpu.VMEM((slot_total, PLEN, cw), BF16),
            pltpu.VMEM((slot_total, PLEN, cw), BF16),
            pltpu.VMEM((st_n, dw, hw), BF16),
            pltpu.VMEM((st_n, dw, hw), BF16),
            pltpu.VMEM((dw, hw), F32),
            sem(2), sem(2), sem(2 * blocks), sem(2 * blocks), sem(2), sem(2 * blocks * (z_n + 1)),
            sem(1), sem(1), sem(1), sem(1), sem(3 + blocks),
        ],
        compiler_params=pltpu.CompilerParams(
            collective_id=0, has_side_effects=True, vmem_limit_bytes=62 << 20
        ),
        name="main",
    )(ids, store, normed, w_q, w_g, w_k, w_v, cot)


def spread_kernel(
    ids_h, returned_h, rows_h, gqw_h, out_h, rows_out, gqw_out,
    ids, returned, rows, gqw, total, in_sem, out_sem, chunk_sem,
):
    slots, passes = ids.shape[0], out_h.shape[0]
    names = pltpu.make_async_copy(ids_h, ids, in_sem.at[3])
    names.start()
    pull = pltpu.make_async_copy(returned_h, returned, in_sem.at[2])
    pull.start()
    sides, loads = [], []
    for i, (far, near, out) in enumerate(((rows_h, rows, rows_out), (gqw_h, gqw, gqw_out))):
        loads.append(pltpu.make_async_copy(far, near, in_sem.at[i]))
        loads[-1].start()
        sides.append(pltpu.make_async_copy(near, out, out_sem.at[i]))
    total[...] = jnp.zeros_like(total)
    names.wait()
    pull.wait()
    for s in range(slots):

        @pl.when(ids[s] >= 0)
        def _():
            total[ids[s]] += returned[s].astype(F32)

    chunks = chunk_sem.shape[0]
    size = passes // chunks
    for i in range(chunks):
        span = slice(i * size, (i + 1) * size)
        sides.append(pltpu.make_async_copy(total.at[span], out_h.at[span], chunk_sem.at[i]))
        sides[-1].start()
    for load, store in zip(loads, sides):
        load.wait()
        store.start()
    for copy in sides:
        copy.wait()


def spread(ids, returned, grad_rows, grad_query_weight, passes):
    width = returned.shape[2]
    hbm = pl.BlockSpec(memory_space=pl.ANY)
    chunks = GROUP if passes % GROUP == 0 else 1
    return pl.pallas_call(
        spread_kernel,
        out_shape=(
            jax.ShapeDtypeStruct((passes, PLEN, width), F32),
            jax.ShapeDtypeStruct(grad_rows.shape, F32),
            jax.ShapeDtypeStruct(grad_query_weight.shape, F32),
        ),
        in_specs=[hbm] * 4,
        out_specs=(hbm,) * 3,
        scratch_shapes=[
            pltpu.SMEM(ids.shape, jnp.int32),
            pltpu.VMEM(returned.shape, BF16),
            pltpu.VMEM(grad_rows.shape, F32),
            pltpu.VMEM(grad_query_weight.shape, F32),
            pltpu.VMEM((passes, PLEN, width), F32),
            pltpu.SemaphoreType.DMA((4,)),
            pltpu.SemaphoreType.DMA((2,)),
            pltpu.SemaphoreType.DMA((chunks,)),
        ],
        compiler_params=pltpu.CompilerParams(vmem_limit_bytes=62 << 20),
        name="spread",
    )(ids, returned, grad_rows, grad_query_weight)


def shards(normed, store, passage_ids, w_query, w_gate, w_key, w_value, cotangent):
    grad_rows, returned, grad_query_weight, served_ids = main_call(
        lax.axis_size("st"), lax.axis_size("tp"), passage_ids.T,
        store.reshape(-1, PLEN, store.shape[1]), normed, w_query, w_gate, w_key, w_value, cotangent,
    )
    grad_store, grad_rows, grad_query_weight = spread(
        served_ids, returned, grad_rows, grad_query_weight, store.shape[0] // PLEN
    )
    return (grad_rows, grad_store.reshape(store.shape[0], -1), grad_query_weight)


def solution(mesh):
    placed = (
        P("st", None),
        P("st", None),
        P("st", None),
        P(None, "tp"),
        P(None, "tp"),
        P(None, "tp"),
        P(None, "tp"),
        P("st", "tp"),
    )
    return jax.shard_map(
        shards,
        mesh=mesh,
        in_specs=placed,
        out_specs=(P("st", "tp"), P("st", "tp"), P("st", "tp")),
        check_vma=False,
    )
```

```python
import functools

import jax
import jax.numpy as jnp
from jax import lax
from jax.experimental import pallas as pl
from jax.experimental.pallas import tpu as pltpu
from jax.sharding import PartitionSpec as P

DH = 128
BLK = 128
PLEN = 64
GROUP = 4
CORES = 2
F32 = jnp.float32
BF16 = jnp.bfloat16
MESH = pl.DeviceIdType.MESH


def dot_nn(a, b):
    return lax.dot_general(a, b, (((1,), (0,)), ((), ())), preferred_element_type=F32)


def dot_nt(a, b):
    return lax.dot_general(a, b, (((1,), (1,)), ((), ())), preferred_element_type=F32)


def dot_tn(a, b):
    return lax.dot_general(a, b, (((0,), (0,)), ((), ())), preferred_element_type=F32)


def rows_at(index, size):
    return pl.ds(pl.multiple_of(index * size, size), size)


def main_kernel(
    st_n, tp_n, reads, slots, pass_dev,
    ids_h, store_h, normed_h, w_q_h, w_g_h, w_k_h, w_v_h, cot_h,
    rows_out, ret_out, gqw_out, served_out,
    store, normed, w_q, w_g, w_k, w_v, cot, load_sem,
    ids, mine, tables, served_ids, req_of, slot_of, early_of, t_ss, t_rs,
    served, arr_e, arr_all, q_s, gate_s, dq_s, dg_s, dp_s,
    x_out, x_in, z_out, up_in, dn_in, own, part, r_out, r_in, g_out, g_in, g_own,
    kv_ss, kv_rs, x_ss, x_rs, z_ss, z_rs, r_ss, r_rs, g_ss, g_rs, out_sem,
):
    me_st, me_tp = lax.axis_index("st"), lax.axis_index("tp")
    z_n = tp_n // CORES
    me_z, me_c = me_tp // CORES, me_tp % CORES
    mate = (me_st, me_z * CORES + 1 - me_c)
    tok, hw = cot.shape
    depth = w_q.shape[0]
    heads = hw // DH
    blocks = tok // BLK
    cw = depth // tp_n
    first = min(reads, slots)
    n_pos = blocks * reads
    scale = DH ** (-0.5)

    def st_peer(d):
        return lax.rem(me_st + d, st_n)

    def st_from(d):
        return lax.rem(me_st + st_n - d, st_n)

    def load(i, far, near):
        copy = pltpu.make_async_copy(far, near, load_sem.at[i])
        copy.start()
        return copy

    ids_load = load(7, ids_h, ids)
    loads_a = [
        load(i, far, near)
        for i, (far, near) in enumerate(((w_k_h, w_k), (store_h, store), (w_v_h, w_v)))
    ]

    above, below = me_z < z_n - 1, me_z > 0
    barrier = pltpu.get_barrier_semaphore()

    def greet(device):
        pl.semaphore_signal(barrier, inc=1, device_id=device, device_id_type=MESH)

    for d in range(1, st_n):
        for c in range(CORES):
            greet((st_peer(d), me_z * CORES + c))

    @pl.when(above)
    def _():
        greet((me_st, (me_z + 1) * CORES + me_c))

    @pl.when(below)
    def _():
        greet((me_st, (me_z - 1) * CORES + me_c))

    greet(mate)

    ids_load.wait()
    passages = [ids[i % reads, i // reads] for i in range(n_pos)]
    owners = [lax.div(p, jnp.int32(pass_dev)) for p in passages]
    ranks = []
    for i in range(n_pos):
        rank = jnp.int32(0)
        for j in range(i):
            rank = rank + jnp.where(owners[j] == owners[i], 1, 0)
        ranks.append(rank)
    places = [owners[i] * slots + ranks[i] for i in range(n_pos)]
    for i in range(n_pos):
        slot_of[i] = places[i]
        early_of[i] = owners[i] * first + jnp.minimum(ranks[i], first - 1)
    for s in range(st_n * slots):
        local, position = jnp.int32(-1), jnp.int32(0)
        for i in range(n_pos):
            hit = places[i] == s
            local = jnp.where(hit, passages[i] - (s // slots) * pass_dev, local)
            position = jnp.where(hit, i, position)
        mine[s] = local
        req_of[s] = position

    def barrier_wait():
        pl.semaphore_wait(
            barrier, CORES * (st_n - 1) + 1 + jnp.where(above, 1, 0) + jnp.where(below, 1, 0)
        )

    barrier_wait()

    def remote(src, dst, ss, rs, dev):
        return pltpu.make_async_remote_copy(
            src_ref=src, dst_ref=dst, send_sem=ss, recv_sem=rs, device_id=dev, device_id_type=MESH
        )

    def landed(ref, rs):
        remote(ref, ref, out_sem.at[0], rs, mate).wait_recv()

    def gone(ref, ss):
        remote(ref, ref, ss, out_sem.at[0], mate).wait_send()

    def table_copy(d, c):
        return remote(
            mine, tables.at[d], t_ss.at[c], t_rs.at[0], (st_peer(d), me_z * CORES + c)
        )

    @pl.when(me_c == CORES - 1)
    def _():
        for c in range(CORES):
            for d in range(1, st_n):
                table_copy(d, c).start()

    loads_b = [
        load(3 + i, far, near)
        for i, (far, near) in enumerate(
            ((normed_h, normed), (w_q_h, w_q), (w_g_h, w_g), (cot_h, cot))
        )
    ]

    def store_wait():
        for copy in loads_a:
            copy.wait()

    def table_wait():
        landed(tables.at[:st_n - 1], t_rs.at[0])

    store_wait()
    table_wait()

    def wanted(d, k):
        at = me_st * slots + k
        return tables[st_n - d, at] if d else mine[at]

    halves = (0, 1)

    def kv_copy(d, k):
        landing = arr_e.at[me_st * first + k] if k < first else arr_all.at[me_st * slots + k]
        source = served.at[d * slots + k]
        late = 0 if k < first else 1
        return remote(source, landing, kv_ss.at[late], kv_rs.at[late], (st_peer(d), me_tp))

    def project(some):
        rows = jnp.concatenate([store[jnp.maximum(wanted(d, k), 0)] for d, k in some], axis=0)
        for half in halves:
            made = dot_nn(rows, (w_k, w_v)[half][...]).astype(BF16)
            for i, (d, k) in enumerate(some):
                piece = made[i * PLEN:(i + 1) * PLEN]
                if d:
                    served[d * slots + k, half] = piece
                elif k < first:
                    arr_e[me_st * first + k, half] = piece
                else:
                    arr_all[me_st * slots + k, half] = piece
        for d, k in some:
            if d and k < first:
                kv_copy(d, k).start()

    far = [(d, k) for k in range(slots) for d in range(1, st_n)]
    size = st_n - 1 if st_n <= GROUP else GROUP
    for i in range(0, len(far), size):
        project(far[i:i + size])
    near = [(0, k) for k in range(slots)]
    for i in range(0, slots, GROUP):
        project(near[i:i + GROUP])

    for d in range(st_n):
        for k in range(slots):
            served_ids[st_peer(d) * slots + k] = wanted(d, k)

    outs = []

    def put(i, near, far):
        copy = pltpu.make_async_copy(near, far, out_sem.at[i])
        copy.start()
        outs.append(copy)

    put(2, served_ids, served_out)
    for copy in loads_b:
        copy.wait()
    tile = 2 * BLK

    @pl.loop(0, tok // tile)
    def _(i):
        span = rows_at(i, tile)
        q_s[span, :] = dot_nn(normed[span, :], w_q[...]).astype(BF16)
        gate_s[span, :] = jax.nn.sigmoid(dot_nn(normed[span, :], w_g[...]))

    late = (st_n - 1) * (slots - first)

    def kv_arrived(phase):
        if phase == 0:
            landed(arr_e.at[:(st_n - 1) * first], kv_rs.at[0])
        else:
            landed(arr_all.at[:late], kv_rs.at[1])

    span = reads * PLEN

    def attend(b):
        if b == 0 or slots == first:
            parts = [arr_e[early_of[b * reads + r]] for r in range(reads)]
        else:
            parts = [arr_all[slot_of[b * reads + r]] for r in range(reads)]
        keys = jnp.concatenate([part[0] for part in parts], axis=0)
        values = jnp.concatenate([part[1] for part in parts], axis=0)
        toks = slice(b * BLK, (b + 1) * BLK)
        ctx = slice(b * span, (b + 1) * span)
        cols = [slice(h * DH, (h + 1) * DH) for h in range(heads)]
        colsv = [slice(hw + h * DH, hw + (h + 1) * DH) for h in range(heads)]
        k = [keys[:, ch] for ch in cols]
        v = [values[:, ch] for ch in cols]
        q = [q_s[toks, ch] for ch in cols]
        gate = [gate_s[toks, ch] for ch in cols]
        up = [cot[toks, ch].astype(F32) for ch in cols]
        each = range(heads)
        s = [dot_nt(q[h], k[h]) * scale for h in each]
        d_att = [(up[h] * gate[h]).astype(BF16) for h in each]
        d_p = [dot_nt(d_att[h], v[h]) for h in each]
        e = [jnp.exp(s[h] - jnp.max(s[h], axis=1, keepdims=True)) for h in each]
        p = [e[h] / jnp.sum(e[h], axis=1, keepdims=True) for h in each]
        low = [p[h].astype(BF16) for h in each]
        delta = [jnp.sum(d_p[h] * p[h], axis=1, keepdims=True) for h in each]
        d_s = [(p[h] * (d_p[h] - delta[h]) * scale).astype(BF16) for h in each]
        d_k = [dot_tn(d_s[h], q[h]) for h in each]
        d_v = [dot_tn(low[h], d_att[h]) for h in each]
        att = [dot_nn(low[h], v[h]) for h in each]
        d_q = [dot_nn(d_s[h], k[h]) for h in each]
        for h in each:
            dp_s[ctx, cols[h]] = d_k[h].astype(BF16)
            dp_s[ctx, colsv[h]] = d_v[h].astype(BF16)
        for h in each:
            dg_s[toks, cols[h]] = (up[h] * att[h] * gate[h] * (1.0 - gate[h])).astype(BF16)
            dq_s[toks, cols[h]] = d_q[h].astype(BF16)

    def chunk(g, t):
        which, b = g
        w_rows = rows_at(t, cw)
        if which == 0:
            ctx = slice(b * span, (b + 1) * span)
            return dot_nt(dp_s[ctx, :hw], w_k[w_rows, :]) + dot_nt(dp_s[ctx, hw:], w_v[w_rows, :])
        toks = slice(b * BLK, (b + 1) * BLK)
        return dot_nt(dq_s[toks, :], w_q[w_rows, :]) + dot_nt(dg_s[toks, :], w_g[w_rows, :])

    order = []
    for i in range((z_n + 1) // 2):
        order += [z_n - 1 - i, i] if z_n - 1 - i != i else [i]

    def piece_of(g, t):
        return (g[0] * blocks + g[1]) * z_n + t

    def all_of(g):
        at = piece_of(g, 0)
        return slice(at, at + z_n)

    batches = [[(0, 0)], [(1, 0)]] + [[(0, b)] for b in range(1, blocks)]
    batches.append([(1, b) for b in range(1, blocks)])
    early_groups = [g for batch in batches[:-1] for g in batch]

    def hop(g, t, up):
        n = piece_of(g, t)
        to = me_z + 1 if up else me_z - 1
        return remote(
            z_out.at[n], (up_in if up else dn_in).at[n],
            z_ss.at[0 if g in early_groups else 1],
            z_rs.at[piece_of(g, 0) // z_n * (z_n + 1) + t + (1 if up else 0)],
            (me_st, to * CORES + me_c),
        )

    def give(g):
        for t in order:
            x_out[piece_of(g, t)] = chunk(g, t * CORES + 1 - me_c).astype(BF16)
        i = piece_of(g, 0) // z_n
        for t in order:
            n = piece_of(g, t)
            remote(x_out.at[n], x_in.at[n], x_ss.at[i], x_rs.at[i], mate).start()

    def take(g):
        for t in order:
            own[piece_of(g, t)] = chunk(g, t * CORES + me_c)
        landed(x_in.at[all_of(g)], x_rs.at[piece_of(g, 0) // z_n])
        for t in order:
            n = piece_of(g, t)
            own[n] = own[n] + x_in[n].astype(F32)

    def depart(batch):
        @pl.when(me_z == 0)
        def _():
            for t in range(z_n - 1, 0, -1):
                for g in batch:
                    n = piece_of(g, t)
                    z_out[n] = own[n].astype(BF16)
                    hop(g, t, True).start()

        @pl.when(me_z == z_n - 1)
        def _():
            for t in range(z_n - 1):
                for g in batch:
                    n = piece_of(g, t)
                    z_out[n] = own[n].astype(BF16)
                    hop(g, t, False).start()

    def pass_on(batch, up, t):
        landing = up_in if up else dn_in
        for g in batch:
            n = piece_of(g, t)
            hop(g, t, up).wait_recv()
            z_out[n] = (own[n] + landing[n].astype(F32)).astype(BF16)
            hop(g, t, up).start()

    def relay(batch, z, stages):
        moves = [(z_n - 1 - t, z, True, t) for t in range(z + 1, z_n)]
        moves += [(t, z_n - 1 - z, False, t) for t in range(z)]
        moves = [m for m in moves if m[1] in stages]

        @pl.when(me_z == z)
        def _():
            for m in sorted(moves, key=lambda m: (m[0] + m[1], -m[1])):
                pass_on(batch, m[2], m[3])

    def gathered(g):
        n = piece_of(g, me_z)

        @pl.when(below)
        def _():
            hop(g, me_z, True).wait_recv()
            own[n] = own[n] + up_in[n].astype(F32)

        @pl.when(above)
        def _():
            hop(g, me_z, False).wait_recv()
            own[n] = own[n] + dn_in[n].astype(F32)

        which, b = g
        if which == 0:
            part[b * reads:(b + 1) * reads] = own[n].astype(BF16).reshape(reads, PLEN, cw)

    reads_end = blocks
    relayed = [0]

    def relay_step():
        j = relayed[0]
        relayed[0] += 1
        for z in range(1, z_n - 1):
            for k in range(1, z_n - 1):
                if 0 <= j - (k - 1) <= reads_end and k in (z, z_n - 1 - z):
                    relay(batches[j - (k - 1)], z, (k,))

    kv_arrived(0)
    for k in range(first, slots):
        for d in range(1, st_n):
            kv_copy(d, k).start()
    attend(0)
    give((0, 0))
    take((0, 0))
    depart(batches[0])
    give((1, 0))
    take((1, 0))
    depart(batches[1])
    if slots > first:
        for o in range(st_n):
            for k in range(first):
                arr_all[o * slots + k] = arr_e[o * first + k]
        kv_arrived(1)

    for b in range(1, blocks):
        attend(b)
        give((0, b))
        if b > 1:
            take((0, b - 1))
            depart([(0, b - 1)])
        if b == 2:
            relay_step()
    for b in range(1, blocks):
        give((1, b))
        if b == 1:
            take((0, blocks - 1))
            depart([(0, blocks - 1)])
            relay_step()
        else:
            take((1, b - 1))
    take((1, blocks - 1))
    depart(batches[-1])
    relay_step()

    dw = depth // st_n
    for d in list(range(1, st_n)) + [0]:
        term = dot_tn(normed[:, rows_at(st_peer(d), dw)], dq_s[...])
        if d == 0:
            g_own[...] = term
        else:
            g_out[d] = term.astype(BF16)
            remote(
                g_out.at[d], g_in.at[d], g_ss.at[0], g_rs.at[0], (st_peer(d), me_tp)
            ).start()

    while relayed[0] < reads_end + 1 + max(z_n - 3, 0):
        relay_step()
    for b in range(blocks):
        gathered((0, b))
    for s in range(st_n * slots):
        r_out[s] = part[req_of[s]]
    for d in range(1, st_n):
        remote(
            r_out.at[rows_at(st_peer(d), slots)], r_in.at[rows_at(me_st, slots)],
            r_ss.at[0], r_rs.at[0], (st_peer(d), me_tp),
        ).start()
    r_in[rows_at(me_st, slots)] = r_out[rows_at(me_st, slots)]

    def gqw_wait():
        total = g_own[...]
        landed(g_in.at[:st_n - 1], g_rs.at[0])
        for d in range(1, st_n):
            total = total + g_in[d].astype(F32)
        g_own[...] = total
        put(1, g_own, gqw_out)

    def send_wait():
        gone(served.at[:(st_n - 1) * first], kv_ss.at[0])
        if slots > first:
            gone(served.at[:late], kv_ss.at[1])
        for g in [g for batch in batches for g in batch]:
            gone(x_out.at[all_of(g)], x_ss.at[piece_of(g, 0) // z_n])
        gone(g_out.at[:st_n - 1], g_ss.at[0])
        gone(z_out.at[:len(early_groups) * (z_n - 1)], z_ss.at[0])

    @pl.when(me_c == CORES - 1)
    def _():
        for c in range(CORES):
            gone(tables.at[:st_n - 1], t_ss.at[c])

    for z in range(1, z_n - 1):
        relay(batches[-1], z, range(z_n))
    gqw_wait()
    send_wait()

    def ret_wait():
        landed(r_in.at[:(st_n - 1) * slots], r_rs.at[0])
        put(0, r_in, ret_out)

    ret_wait()
    for b in range(blocks):
        gathered((1, b))
        put(3 + b, own.at[piece_of((1, b), me_z)], rows_out.at[b * BLK:(b + 1) * BLK])
    gone(z_out.at[:len(batches[-1]) * (z_n - 1)], z_ss.at[1])
    gone(r_out.at[:(st_n - 1) * slots], r_ss.at[0])

    def out_wait():
        for copy in outs:
            copy.wait()

    out_wait()


def main_call(st_n, tp_n, ids, store, normed, w_q, w_g, w_k, w_v, cot):
    reads, blocks = ids.shape
    tok, hw = cot.shape
    depth = w_q.shape[0]
    cw, dw, z_n = depth // tp_n, depth // st_n, tp_n // CORES
    pass_dev = store.shape[0]
    n_pos = blocks * reads
    slots = max(1, 2 * n_pos // st_n)
    first = min(reads, slots)
    ctx = blocks * reads * PLEN
    slot_total = st_n * slots
    hbm = pl.BlockSpec(memory_space=pl.ANY)
    pieces = 2 * blocks * z_n
    piece = lambda kind=BF16: pltpu.VMEM((pieces, BLK, cw), kind)
    sem = lambda n: pltpu.SemaphoreType.DMA((n,))
    table = lambda *n: pltpu.SMEM(n, jnp.int32)
    assert ctx == tok
    return pl.pallas_call(
        functools.partial(main_kernel, st_n, tp_n, reads, slots, pass_dev),
        out_shape=(
            jax.ShapeDtypeStruct((tok, cw), F32),
            jax.ShapeDtypeStruct((slot_total, PLEN, cw), BF16),
            jax.ShapeDtypeStruct((dw, hw), F32),
            jax.ShapeDtypeStruct((slot_total,), jnp.int32),
        ),
        in_specs=[hbm] * 8,
        out_specs=(hbm, hbm, hbm, hbm),
        scratch_shapes=[
            *[pltpu.VMEM(a.shape, a.dtype) for a in (store, normed, w_q, w_g, w_k, w_v, cot)],
            sem(8),
            table(*ids.shape), table(slot_total), table(st_n, slot_total), table(slot_total),
            table(slot_total), table(n_pos), table(n_pos),
            sem(CORES), sem(1),
            pltpu.VMEM((slot_total, 2, PLEN, hw), BF16),
            pltpu.VMEM((st_n * first, 2, PLEN, hw), BF16),
            pltpu.VMEM((slot_total, 2, PLEN, hw), BF16),
            pltpu.VMEM((tok, hw), BF16),
            pltpu.VMEM((tok, hw), F32),
            pltpu.VMEM((tok, hw), BF16),
            pltpu.VMEM((tok, hw), BF16),
            pltpu.VMEM((ctx, 2 * hw), BF16),
            piece(), piece(), piece(), piece(), piece(), piece(F32),
            pltpu.VMEM((ctx // PLEN, PLEN, cw), BF16),
            pltpu.VMEM((slot_total, PLEN, cw), BF16),
            pltpu.VMEM((slot_total, PLEN, cw), BF16),
            pltpu.VMEM((st_n, dw, hw), BF16),
            pltpu.VMEM((st_n, dw, hw), BF16),
            pltpu.VMEM((dw, hw), F32),
            sem(2), sem(2), sem(2 * blocks), sem(2 * blocks), sem(2), sem(2 * blocks * (z_n + 1)),
            sem(1), sem(1), sem(1), sem(1), sem(3 + blocks),
        ],
        compiler_params=pltpu.CompilerParams(
            collective_id=0, has_side_effects=True, vmem_limit_bytes=46 << 20
        ),
        name="main",
    )(*[
        pltpu.with_memory_space_constraint(a, pltpu.HBM)
        for a in (ids, store, normed, w_q, w_g, w_k, w_v, cot)
    ])


def spread_kernel(
    ids_h, returned, rows, gqw, out_h, rows_out, gqw_out, ids, total, sems, chunk_sem,
):
    slots, passes = ids.shape[0], out_h.shape[0]
    names = pltpu.make_async_copy(ids_h, ids, sems.at[2])
    names.start()
    outs = [
        pltpu.make_async_copy(near, far, sems.at[i])
        for i, (near, far) in enumerate(((rows, rows_out), (gqw, gqw_out)))
    ]
    for copy in outs:
        copy.start()
    total[...] = jnp.zeros_like(total)
    names.wait()
    for s in range(slots):

        @pl.when(ids[s] >= 0)
        def _():
            total[ids[s]] += returned[s].astype(F32)

    chunks = chunk_sem.shape[0]
    size = passes // chunks
    for i in range(chunks):
        span = slice(i * size, (i + 1) * size)
        outs.append(pltpu.make_async_copy(total.at[span], out_h.at[span], chunk_sem.at[i]))
        outs[-1].start()
    for copy in outs:
        copy.wait()


def spread(ids, returned, grad_rows, grad_query_weight, passes):
    width = returned.shape[2]
    hbm = pl.BlockSpec(memory_space=pl.ANY)
    vmem = pl.BlockSpec(memory_space=pltpu.VMEM)
    chunks = GROUP if passes % GROUP == 0 else 1
    return pl.pallas_call(
        spread_kernel,
        out_shape=(
            jax.ShapeDtypeStruct((passes, PLEN, width), F32),
            jax.ShapeDtypeStruct(grad_rows.shape, F32),
            jax.ShapeDtypeStruct(grad_query_weight.shape, F32),
        ),
        in_specs=[hbm] + [vmem] * 3,
        out_specs=(hbm,) * 3,
        scratch_shapes=[
            pltpu.SMEM(ids.shape, jnp.int32),
            pltpu.VMEM((passes, PLEN, width), F32),
            pltpu.SemaphoreType.DMA((3,)),
            pltpu.SemaphoreType.DMA((chunks,)),
        ],
        compiler_params=pltpu.CompilerParams(vmem_limit_bytes=8 << 20),
        name="spread",
    )(ids, returned, grad_rows, grad_query_weight)


def shards(normed, store, passage_ids, w_query, w_gate, w_key, w_value, cotangent):
    grad_rows, returned, grad_query_weight, served_ids = main_call(
        lax.axis_size("st"), lax.axis_size("tp"), passage_ids.T,
        store.reshape(-1, PLEN, store.shape[1]), normed, w_query, w_gate, w_key, w_value, cotangent,
    )
    grad_store, grad_rows, grad_query_weight = spread(
        served_ids, returned, grad_rows, grad_query_weight, store.shape[0] // PLEN
    )
    return (grad_rows, grad_store.reshape(store.shape[0], -1), grad_query_weight)


def solution(mesh):
    placed = (
        P("st", None),
        P("st", None),
        P("st", None),
        P(None, "tp"),
        P(None, "tp"),
        P(None, "tp"),
        P(None, "tp"),
        P("st", "tp"),
    )
    return jax.shard_map(
        shards,
        mesh=mesh,
        in_specs=placed,
        out_specs=(P("st", "tp"), P("st", "tp"), P("st", "tp")),
        check_vma=False,
    )
```

```python
import functools

import jax
import jax.numpy as jnp
from jax import lax
from jax.experimental import pallas as pl
from jax.experimental.pallas import tpu as pltpu
from jax.sharding import PartitionSpec as P

DH = 128
BLK = 128
PLEN = 64
GROUP = 4
CORES = 2
F32 = jnp.float32
BF16 = jnp.bfloat16
MESH = pl.DeviceIdType.MESH


def dot_nn(a, b):
    return lax.dot_general(a, b, (((1,), (0,)), ((), ())), preferred_element_type=F32)


def dot_nt(a, b):
    return lax.dot_general(a, b, (((1,), (1,)), ((), ())), preferred_element_type=F32)


def dot_tn(a, b):
    return lax.dot_general(a, b, (((0,), (0,)), ((), ())), preferred_element_type=F32)


def rows_at(index, size):
    return pl.ds(pl.multiple_of(index * size, size), size)


def main_kernel(
    st_n, tp_n, reads, slots, pass_dev,
    ids_h, store_h, normed_h, w_q_h, w_g_h, w_k_h, w_v_h, cot_h,
    rows_out, ret_out, gqw_out, served_out,
    store, normed, w_q, w_g, w_k, w_v, cot, load_sem,
    ids, mine, tables, served_ids, req_of, slot_of, early_of, t_ss, t_rs,
    served, arr_e, arr_all, q_s, gate_s, dq_s, dg_s, dp_s,
    x_out, x_in, z_out, up_in, dn_in, own, part, r_out, r_in, g_out, g_in, g_own,
    kv_ss, kv_rs, x_ss, x_rs, z_ss, z_rs, r_ss, r_rs, g_ss, g_rs, out_sem,
):
    me_st, me_tp = lax.axis_index("st"), lax.axis_index("tp")
    z_n = tp_n // CORES
    me_z, me_c = me_tp // CORES, me_tp % CORES
    mate = (me_st, me_z * CORES + 1 - me_c)
    tok, hw = cot.shape
    depth = w_q.shape[0]
    heads = hw // DH
    blocks = tok // BLK
    cw = depth // tp_n
    first = min(reads, slots)
    n_pos = blocks * reads
    scale = DH ** (-0.5)

    def st_peer(d):
        return lax.rem(me_st + d, st_n)

    def st_from(d):
        return lax.rem(me_st + st_n - d, st_n)

    def load(i, far, near):
        copy = pltpu.make_async_copy(far, near, load_sem.at[i])
        copy.start()
        return copy

    ids_load = load(7, ids_h, ids)
    loads_a = [
        load(i, far, near)
        for i, (far, near) in enumerate(((w_k_h, w_k), (store_h, store), (w_v_h, w_v)))
    ]

    above, below = me_z < z_n - 1, me_z > 0
    barrier = pltpu.get_barrier_semaphore()

    def greet(device):
        pl.semaphore_signal(barrier, inc=1, device_id=device, device_id_type=MESH)

    for d in range(1, st_n):
        for c in range(CORES):
            greet((st_peer(d), me_z * CORES + c))

    @pl.when(above)
    def _():
        greet((me_st, (me_z + 1) * CORES + me_c))

    @pl.when(below)
    def _():
        greet((me_st, (me_z - 1) * CORES + me_c))

    greet(mate)

    ids_load.wait()
    passages = [ids[i % reads, i // reads] for i in range(n_pos)]
    owners = [lax.div(p, jnp.int32(pass_dev)) for p in passages]
    ranks = []
    for i in range(n_pos):
        rank = jnp.int32(0)
        for j in range(i):
            rank = rank + jnp.where(owners[j] == owners[i], 1, 0)
        ranks.append(rank)
    places = [owners[i] * slots + ranks[i] for i in range(n_pos)]
    for i in range(n_pos):
        slot_of[i] = places[i]
        early_of[i] = owners[i] * first + jnp.minimum(ranks[i], first - 1)
    for s in range(st_n * slots):
        local, position = jnp.int32(-1), jnp.int32(0)
        for i in range(n_pos):
            hit = places[i] == s
            local = jnp.where(hit, passages[i] - (s // slots) * pass_dev, local)
            position = jnp.where(hit, i, position)
        mine[s] = local
        req_of[s] = position

    def barrier_wait():
        pl.semaphore_wait(
            barrier, CORES * (st_n - 1) + 1 + jnp.where(above, 1, 0) + jnp.where(below, 1, 0)
        )

    barrier_wait()

    def remote(src, dst, ss, rs, dev):
        return pltpu.make_async_remote_copy(
            src_ref=src, dst_ref=dst, send_sem=ss, recv_sem=rs, device_id=dev, device_id_type=MESH
        )

    def landed(ref, rs):
        remote(ref, ref, out_sem.at[0], rs, mate).wait_recv()

    def gone(ref, ss):
        remote(ref, ref, ss, out_sem.at[0], mate).wait_send()

    def table_copy(d, c):
        return remote(
            mine, tables.at[d], t_ss.at[c], t_rs.at[0], (st_peer(d), me_z * CORES + c)
        )

    @pl.when(me_c == CORES - 1)
    def _():
        for c in range(CORES):
            for d in range(1, st_n):
                table_copy(d, c).start()

    loads_b = [
        load(3 + i, far, near)
        for i, (far, near) in enumerate(
            ((normed_h, normed), (w_q_h, w_q), (w_g_h, w_g), (cot_h, cot))
        )
    ]

    def store_wait():
        for copy in loads_a:
            copy.wait()

    def table_wait():
        landed(tables.at[:st_n - 1], t_rs.at[0])

    store_wait()
    table_wait()

    def wanted(i, k):
        at = me_st * slots + k
        return tables[st_n - reach(i), at] if i else mine[at]

    def reach(i):
        return jnp.where(lax.rem(me_st, 2) == 0, st_n - i, i) if i else 0

    halves = (0, 1)

    def kv_copy(d, k):
        landing = arr_e.at[me_st * first + k] if k < first else arr_all.at[me_st * slots + k]
        source = served.at[d * slots + k]
        late = 0 if k < first else 1
        return remote(
            source, landing, kv_ss.at[late], kv_rs.at[late], (st_peer(reach(d)), me_tp)
        )

    def project(some):
        rows = jnp.concatenate([store[jnp.maximum(wanted(d, k), 0)] for d, k in some], axis=0)
        for half in halves:
            made = dot_nn(rows, (w_k, w_v)[half][...]).astype(BF16)
            for i, (d, k) in enumerate(some):
                piece = made[i * PLEN:(i + 1) * PLEN]
                if d:
                    served[d * slots + k, half] = piece
                elif k < first:
                    arr_e[me_st * first + k, half] = piece
                else:
                    arr_all[me_st * slots + k, half] = piece
        for d, k in some:
            if d and k < first:
                kv_copy(d, k).start()

    far = [(d, k) for k in range(slots) for d in range(1, st_n)]
    size = st_n - 1 if st_n <= GROUP else GROUP
    for i in range(0, len(far), size):
        project(far[i:i + size])
    near = [(0, k) for k in range(slots)]
    for i in range(0, slots, GROUP):
        project(near[i:i + GROUP])

    for d in range(st_n):
        for k in range(slots):
            served_ids[st_peer(reach(d)) * slots + k] = wanted(d, k)

    outs = []

    def put(i, near, far):
        copy = pltpu.make_async_copy(near, far, out_sem.at[i])
        copy.start()
        outs.append(copy)

    put(2, served_ids, served_out)
    for copy in loads_b:
        copy.wait()
    tile = 2 * BLK

    @pl.loop(0, tok // tile)
    def _(i):
        span = rows_at(i, tile)
        q_s[span, :] = dot_nn(normed[span, :], w_q[...]).astype(BF16)
        gate_s[span, :] = jax.nn.sigmoid(dot_nn(normed[span, :], w_g[...]))

    late = (st_n - 1) * (slots - first)

    def kv_arrived(phase):
        if phase == 0:
            landed(arr_e.at[:(st_n - 1) * first], kv_rs.at[0])
        else:
            landed(arr_all.at[:late], kv_rs.at[1])

    span = reads * PLEN

    def attend(b):
        if b == 0 or slots == first:
            parts = [arr_e[early_of[b * reads + r]] for r in range(reads)]
        else:
            parts = [arr_all[slot_of[b * reads + r]] for r in range(reads)]
        keys = jnp.concatenate([part[0] for part in parts], axis=0)
        values = jnp.concatenate([part[1] for part in parts], axis=0)
        toks = slice(b * BLK, (b + 1) * BLK)
        ctx = slice(b * span, (b + 1) * span)
        cols = [slice(h * DH, (h + 1) * DH) for h in range(heads)]
        colsv = [slice(hw + h * DH, hw + (h + 1) * DH) for h in range(heads)]
        k = [keys[:, ch] for ch in cols]
        v = [values[:, ch] for ch in cols]
        q = [q_s[toks, ch] for ch in cols]
        gate = [gate_s[toks, ch] for ch in cols]
        up = [cot[toks, ch].astype(F32) for ch in cols]
        each = range(heads)
        s = [dot_nt(q[h], k[h]) * scale for h in each]
        d_att = [(up[h] * gate[h]).astype(BF16) for h in each]
        d_p = [dot_nt(d_att[h], v[h]) for h in each]
        e = [jnp.exp(s[h] - jnp.max(s[h], axis=1, keepdims=True)) for h in each]
        p = [e[h] / jnp.sum(e[h], axis=1, keepdims=True) for h in each]
        low = [p[h].astype(BF16) for h in each]
        delta = [jnp.sum(d_p[h] * p[h], axis=1, keepdims=True) for h in each]
        d_s = [(p[h] * (d_p[h] - delta[h]) * scale).astype(BF16) for h in each]
        d_k = [dot_tn(d_s[h], q[h]) for h in each]
        d_v = [dot_tn(low[h], d_att[h]) for h in each]
        att = [dot_nn(low[h], v[h]) for h in each]
        d_q = [dot_nn(d_s[h], k[h]) for h in each]
        for h in each:
            dp_s[ctx, cols[h]] = d_k[h].astype(BF16)
            dp_s[ctx, colsv[h]] = d_v[h].astype(BF16)
        for h in each:
            dg_s[toks, cols[h]] = (up[h] * att[h] * gate[h] * (1.0 - gate[h])).astype(BF16)
            dq_s[toks, cols[h]] = d_q[h].astype(BF16)

    def chunk(g, t):
        which, b = g
        w_rows = rows_at(t, cw)
        if which == 0:
            ctx = slice(b * span, (b + 1) * span)
            return dot_nt(dp_s[ctx, :hw], w_k[w_rows, :]) + dot_nt(dp_s[ctx, hw:], w_v[w_rows, :])
        toks = slice(b * BLK, (b + 1) * BLK)
        return dot_nt(dq_s[toks, :], w_q[w_rows, :]) + dot_nt(dg_s[toks, :], w_g[w_rows, :])

    order = []
    for i in range((z_n + 1) // 2):
        order += [z_n - 1 - i, i] if z_n - 1 - i != i else [i]

    def piece_of(g, t):
        return (g[0] * blocks + g[1]) * z_n + t

    def all_of(g):
        at = piece_of(g, 0)
        return slice(at, at + z_n)

    batches = [[(0, 0)], [(1, 0)]] + [[(0, b)] for b in range(1, blocks)]
    batches.append([(1, b) for b in range(1, blocks)])
    early_groups = [g for batch in batches[:-1] for g in batch]

    def hop(g, t, up):
        n = piece_of(g, t)
        to = me_z + 1 if up else me_z - 1
        return remote(
            z_out.at[n], (up_in if up else dn_in).at[n],
            z_ss.at[0 if g in early_groups else 1],
            z_rs.at[piece_of(g, 0) // z_n * (z_n + 1) + t + (1 if up else 0)],
            (me_st, to * CORES + me_c),
        )

    def give(g):
        for t in order:
            x_out[piece_of(g, t)] = chunk(g, t * CORES + 1 - me_c).astype(BF16)
        i = piece_of(g, 0) // z_n
        for t in order:
            n = piece_of(g, t)
            remote(x_out.at[n], x_in.at[n], x_ss.at[0], x_rs.at[i], mate).start()

    def take(g):
        for t in order:
            own[piece_of(g, t)] = chunk(g, t * CORES + me_c)
        landed(x_in.at[all_of(g)], x_rs.at[piece_of(g, 0) // z_n])
        for t in order:
            n = piece_of(g, t)
            own[n] = own[n] + x_in[n].astype(F32)

    def depart(batch):
        @pl.when(me_z == 0)
        def _():
            for t in range(z_n - 1, 0, -1):
                for g in batch:
                    n = piece_of(g, t)
                    z_out[n] = own[n].astype(BF16)
                    hop(g, t, True).start()

        @pl.when(me_z == z_n - 1)
        def _():
            for t in range(z_n - 1):
                for g in batch:
                    n = piece_of(g, t)
                    z_out[n] = own[n].astype(BF16)
                    hop(g, t, False).start()

    def pass_on(batch, up, t):
        landing = up_in if up else dn_in
        for g in batch:
            n = piece_of(g, t)
            hop(g, t, up).wait_recv()
            z_out[n] = (own[n] + landing[n].astype(F32)).astype(BF16)
            hop(g, t, up).start()

    def relay(batch, z, stages):
        moves = [(z_n - 1 - t, z, True, t) for t in range(z + 1, z_n)]
        moves += [(t, z_n - 1 - z, False, t) for t in range(z)]
        moves = [m for m in moves if m[1] in stages]

        @pl.when(me_z == z)
        def _():
            for m in sorted(moves, key=lambda m: (m[0] + m[1], -m[1])):
                pass_on(batch, m[2], m[3])

    def gathered(g):
        n = piece_of(g, me_z)

        @pl.when(below)
        def _():
            hop(g, me_z, True).wait_recv()
            own[n] = own[n] + up_in[n].astype(F32)

        @pl.when(above)
        def _():
            hop(g, me_z, False).wait_recv()
            own[n] = own[n] + dn_in[n].astype(F32)

        which, b = g
        if which == 0:
            part[b * reads:(b + 1) * reads] = own[n].astype(BF16).reshape(reads, PLEN, cw)

    reads_end = blocks
    relayed = [0]

    def relay_step():
        j = relayed[0]
        relayed[0] += 1
        for z in range(1, z_n - 1):
            for k in range(1, z_n - 1):
                if 0 <= j - (k - 1) <= reads_end and k in (z, z_n - 1 - z):
                    relay(batches[j - (k - 1)], z, (k,))

    kv_arrived(0)
    for k in range(first, slots):
        for d in range(1, st_n):
            kv_copy(d, k).start()
    attend(0)
    give((0, 0))
    take((0, 0))
    depart(batches[0])
    give((1, 0))
    take((1, 0))
    depart(batches[1])
    if slots > first:
        for o in range(st_n):
            for k in range(first):
                arr_all[o * slots + k] = arr_e[o * first + k]
        kv_arrived(1)

    for b in range(1, blocks):
        attend(b)
        give((0, b))
        if b > 1:
            take((0, b - 1))
            depart([(0, b - 1)])
        if b == 2:
            relay_step()
    for b in range(1, blocks):
        give((1, b))
        if b == 1:
            take((0, blocks - 1))
            depart([(0, blocks - 1)])
            relay_step()
        else:
            take((1, b - 1))
    take((1, blocks - 1))
    depart(batches[-1])
    relay_step()

    dw = depth // st_n
    for d in list(range(1, st_n)) + [0]:
        term = dot_tn(normed[:, rows_at(st_peer(d), dw)], dq_s[...])
        if d == 0:
            g_own[...] = term
        else:
            g_out[d] = term.astype(BF16)
            remote(
                g_out.at[d], g_in.at[d], g_ss.at[0], g_rs.at[0], (st_peer(d), me_tp)
            ).start()

    while relayed[0] < reads_end + 1 + max(z_n - 3, 0):
        relay_step()
    for b in range(blocks):
        gathered((0, b))
    for s in range(st_n * slots):
        r_out[s] = part[req_of[s]]
    for d in range(1, st_n):
        remote(
            r_out.at[rows_at(st_peer(d), slots)], r_in.at[rows_at(me_st, slots)],
            r_ss.at[0], r_rs.at[0], (st_peer(d), me_tp),
        ).start()
    r_in[rows_at(me_st, slots)] = r_out[rows_at(me_st, slots)]

    def gqw_wait():
        total = g_own[...]
        landed(g_in.at[:st_n - 1], g_rs.at[0])
        for d in range(1, st_n):
            total = total + g_in[d].astype(F32)
        g_own[...] = total
        put(1, g_own, gqw_out)

    def send_wait():
        gone(served.at[:(st_n - 1) * first], kv_ss.at[0])
        if slots > first:
            gone(served.at[:late], kv_ss.at[1])
        gone(x_out, x_ss.at[0])
        gone(g_out.at[:st_n - 1], g_ss.at[0])
        gone(z_out.at[:len(early_groups) * (z_n - 1)], z_ss.at[0])

    @pl.when(me_c == CORES - 1)
    def _():
        for c in range(CORES):
            gone(tables.at[:st_n - 1], t_ss.at[c])

    for z in range(1, z_n - 1):
        relay(batches[-1], z, range(z_n))
    gqw_wait()
    send_wait()

    def ret_wait():
        landed(r_in.at[:(st_n - 1) * slots], r_rs.at[0])
        put(0, r_in, ret_out)

    ret_wait()
    for b in range(blocks):
        gathered((1, b))
        put(3 + b, own.at[piece_of((1, b), me_z)], rows_out.at[b * BLK:(b + 1) * BLK])
    gone(z_out.at[:len(batches[-1]) * (z_n - 1)], z_ss.at[1])
    gone(r_out.at[:(st_n - 1) * slots], r_ss.at[0])

    def out_wait():
        for copy in outs:
            copy.wait()

    out_wait()


def main_call(st_n, tp_n, ids, store, normed, w_q, w_g, w_k, w_v, cot):
    reads, blocks = ids.shape
    tok, hw = cot.shape
    depth = w_q.shape[0]
    cw, dw, z_n = depth // tp_n, depth // st_n, tp_n // CORES
    pass_dev = store.shape[0]
    n_pos = blocks * reads
    slots = max(1, 2 * n_pos // st_n)
    first = min(reads, slots)
    ctx = blocks * reads * PLEN
    slot_total = st_n * slots
    hbm = pl.BlockSpec(memory_space=pl.ANY)
    pieces = 2 * blocks * z_n
    piece = lambda kind=BF16: pltpu.VMEM((pieces, BLK, cw), kind)
    sem = lambda n: pltpu.SemaphoreType.DMA((n,))
    table = lambda *n: pltpu.SMEM(n, jnp.int32)
    assert ctx == tok
    return pl.pallas_call(
        functools.partial(main_kernel, st_n, tp_n, reads, slots, pass_dev),
        out_shape=(
            jax.ShapeDtypeStruct((tok, cw), F32),
            jax.ShapeDtypeStruct((slot_total, PLEN, cw), BF16),
            jax.ShapeDtypeStruct((dw, hw), F32),
            jax.ShapeDtypeStruct((slot_total,), jnp.int32),
        ),
        in_specs=[hbm] * 8,
        out_specs=(hbm, hbm, hbm, hbm),
        scratch_shapes=[
            *[pltpu.VMEM(a.shape, a.dtype) for a in (store, normed, w_q, w_g, w_k, w_v, cot)],
            sem(8),
            table(*ids.shape), table(slot_total), table(st_n, slot_total), table(slot_total),
            table(slot_total), table(n_pos), table(n_pos),
            sem(CORES), sem(1),
            pltpu.VMEM((slot_total, 2, PLEN, hw), BF16),
            pltpu.VMEM((st_n * first, 2, PLEN, hw), BF16),
            pltpu.VMEM((slot_total, 2, PLEN, hw), BF16),
            pltpu.VMEM((tok, hw), BF16),
            pltpu.VMEM((tok, hw), F32),
            pltpu.VMEM((tok, hw), BF16),
            pltpu.VMEM((tok, hw), BF16),
            pltpu.VMEM((ctx, 2 * hw), BF16),
            piece(), piece(), piece(), piece(), piece(), piece(F32),
            pltpu.VMEM((ctx // PLEN, PLEN, cw), BF16),
            pltpu.VMEM((slot_total, PLEN, cw), BF16),
            pltpu.VMEM((slot_total, PLEN, cw), BF16),
            pltpu.VMEM((st_n, dw, hw), BF16),
            pltpu.VMEM((st_n, dw, hw), BF16),
            pltpu.VMEM((dw, hw), F32),
            sem(2), sem(2), sem(1), sem(2 * blocks), sem(2), sem(2 * blocks * (z_n + 1)),
            sem(1), sem(1), sem(1), sem(1), sem(3 + blocks),
        ],
        compiler_params=pltpu.CompilerParams(
            collective_id=0, has_side_effects=True, vmem_limit_bytes=46 << 20
        ),
        name="main",
    )(*[
        pltpu.with_memory_space_constraint(a, pltpu.HBM)
        for a in (ids, store, normed, w_q, w_g, w_k, w_v, cot)
    ])


def spread_kernel(
    ids_h, returned, rows, gqw, out_h, rows_out, gqw_out, ids, total, sems, chunk_sem,
):
    slots, passes = ids.shape[0], out_h.shape[0]
    names = pltpu.make_async_copy(ids_h, ids, sems.at[2])
    names.start()
    outs = [
        pltpu.make_async_copy(near, far, sems.at[i])
        for i, (near, far) in enumerate(((rows, rows_out), (gqw, gqw_out)))
    ]
    for copy in outs:
        copy.start()
    total[...] = jnp.zeros_like(total)
    names.wait()
    for s in range(slots):

        @pl.when(ids[s] >= 0)
        def _():
            total[ids[s]] += returned[s].astype(F32)

    chunks = chunk_sem.shape[0]
    size = passes // chunks
    for i in range(chunks):
        span = slice(i * size, (i + 1) * size)
        outs.append(pltpu.make_async_copy(total.at[span], out_h.at[span], chunk_sem.at[i]))
        outs[-1].start()
    for copy in outs:
        copy.wait()


def spread(ids, returned, grad_rows, grad_query_weight, passes):
    width = returned.shape[2]
    hbm = pl.BlockSpec(memory_space=pl.ANY)
    vmem = pl.BlockSpec(memory_space=pltpu.VMEM)
    chunks = GROUP if passes % GROUP == 0 else 1
    return pl.pallas_call(
        spread_kernel,
        out_shape=(
            jax.ShapeDtypeStruct((passes, PLEN, width), F32),
            jax.ShapeDtypeStruct(grad_rows.shape, F32),
            jax.ShapeDtypeStruct(grad_query_weight.shape, F32),
        ),
        in_specs=[hbm] + [vmem] * 3,
        out_specs=(hbm,) * 3,
        scratch_shapes=[
            pltpu.SMEM(ids.shape, jnp.int32),
            pltpu.VMEM((passes, PLEN, width), F32),
            pltpu.SemaphoreType.DMA((3,)),
            pltpu.SemaphoreType.DMA((chunks,)),
        ],
        compiler_params=pltpu.CompilerParams(vmem_limit_bytes=8 << 20),
        name="spread",
    )(ids, returned, grad_rows, grad_query_weight)


def shards(normed, store, passage_ids, w_query, w_gate, w_key, w_value, cotangent):
    grad_rows, returned, grad_query_weight, served_ids = main_call(
        lax.axis_size("st"), lax.axis_size("tp"), passage_ids.T,
        store.reshape(-1, PLEN, store.shape[1]), normed, w_query, w_gate, w_key, w_value, cotangent,
    )
    grad_store, grad_rows, grad_query_weight = spread(
        served_ids, returned, grad_rows, grad_query_weight, store.shape[0] // PLEN
    )
    return (grad_rows, grad_store.reshape(store.shape[0], -1), grad_query_weight)


def solution(mesh):
    placed = (
        P("st", None),
        P("st", None),
        P("st", None),
        P(None, "tp"),
        P(None, "tp"),
        P(None, "tp"),
        P(None, "tp"),
        P("st", "tp"),
    )
    return jax.shard_map(
        shards,
        mesh=mesh,
        in_specs=placed,
        out_specs=(P("st", "tp"), P("st", "tp"), P("st", "tp")),
        check_vma=False,
    )
```

```python
import functools

import jax
import jax.numpy as jnp
from jax import lax
from jax.experimental import pallas as pl
from jax.experimental.pallas import tpu as pltpu
from jax.sharding import PartitionSpec as P

DH = 128
BLK = 128
PLEN = 64
GROUP = 4
CORES = 2
F32 = jnp.float32
BF16 = jnp.bfloat16
MESH = pl.DeviceIdType.MESH


def dot_nn(a, b):
    return lax.dot_general(a, b, (((1,), (0,)), ((), ())), preferred_element_type=F32)


def dot_nt(a, b):
    return lax.dot_general(a, b, (((1,), (1,)), ((), ())), preferred_element_type=F32)


def dot_tn(a, b):
    return lax.dot_general(a, b, (((0,), (0,)), ((), ())), preferred_element_type=F32)


def rows_at(index, size):
    return pl.ds(pl.multiple_of(index * size, size), size)


def main_kernel(
    st_n, tp_n, reads, slots, pass_dev,
    ids_h, store_h, normed_h, w_q_h, w_g_h, w_k_h, w_v_h, cot_h,
    rows_out, ret_out, gqw_out, served_out,
    store, normed, w_q, w_g, w_k, w_v, cot, load_sem,
    ids, mine, tables, served_ids, req_of, slot_of, early_of, t_ss, t_rs,
    served, arr_e, arr_all, q_s, gate_s, dq_s, dg_s, dp_s,
    x_out, x_in, z_out, up_in, dn_in, own, part, r_out, r_in, g_out, g_in, g_own,
    kv_ss, kv_rs, x_ss, x_rs, z_ss, z_rs, r_ss, r_rs, g_ss, g_rs, out_sem,
):
    me_st, me_tp = lax.axis_index("st"), lax.axis_index("tp")
    z_n = tp_n // CORES
    me_z, me_c = me_tp // CORES, me_tp % CORES
    mate = (me_st, me_z * CORES + 1 - me_c)
    tok, hw = cot.shape
    depth = w_q.shape[0]
    heads = hw // DH
    blocks = tok // BLK
    cw = depth // tp_n
    first = min(reads, slots)
    n_pos = blocks * reads
    scale = DH ** (-0.5)

    def st_peer(d):
        return lax.rem(me_st + d, st_n)

    def st_from(d):
        return lax.rem(me_st + st_n - d, st_n)

    def load(i, far, near):
        copy = pltpu.make_async_copy(far, near, load_sem.at[i])
        copy.start()
        return copy

    ids_load = load(7, ids_h, ids)
    loads_a = [
        load(i, far, near)
        for i, (far, near) in enumerate(((w_k_h, w_k), (store_h, store), (w_v_h, w_v)))
    ]

    above, below = me_z < z_n - 1, me_z > 0
    barrier = pltpu.get_barrier_semaphore()

    def greet(device):
        pl.semaphore_signal(barrier, inc=1, device_id=device, device_id_type=MESH)

    for d in range(1, st_n):
        for c in range(CORES):
            greet((st_peer(d), me_z * CORES + c))

    @pl.when(above)
    def _():
        greet((me_st, (me_z + 1) * CORES + me_c))

    @pl.when(below)
    def _():
        greet((me_st, (me_z - 1) * CORES + me_c))

    greet(mate)

    ids_load.wait()
    passages = [ids[i % reads, i // reads] for i in range(n_pos)]
    owners = [lax.div(p, jnp.int32(pass_dev)) for p in passages]
    ranks = []
    for i in range(n_pos):
        rank = jnp.int32(0)
        for j in range(i):
            rank = rank + jnp.where(owners[j] == owners[i], 1, 0)
        ranks.append(rank)
    places = [owners[i] * slots + ranks[i] for i in range(n_pos)]
    for i in range(n_pos):
        slot_of[i] = places[i]
        early_of[i] = owners[i] * first + jnp.minimum(ranks[i], first - 1)
    for s in range(st_n * slots):
        local, position = jnp.int32(-1), jnp.int32(0)
        for i in range(n_pos):
            hit = places[i] == s
            local = jnp.where(hit, passages[i] - (s // slots) * pass_dev, local)
            position = jnp.where(hit, i, position)
        mine[s] = local
        req_of[s] = position

    def barrier_wait():
        pl.semaphore_wait(
            barrier, CORES * (st_n - 1) + 1 + jnp.where(above, 1, 0) + jnp.where(below, 1, 0)
        )

    barrier_wait()

    def remote(src, dst, ss, rs, dev):
        return pltpu.make_async_remote_copy(
            src_ref=src, dst_ref=dst, send_sem=ss, recv_sem=rs, device_id=dev, device_id_type=MESH
        )

    def landed(ref, rs):
        remote(ref, ref, out_sem.at[0], rs, mate).wait_recv()

    def gone(ref, ss):
        remote(ref, ref, ss, out_sem.at[0], mate).wait_send()

    def table_copy(d, c):
        return remote(
            mine, tables.at[d], t_ss.at[c], t_rs.at[0], (st_peer(d), me_z * CORES + c)
        )

    @pl.when(me_c == CORES - 1)
    def _():
        for c in range(CORES):
            for d in range(1, st_n):
                table_copy(d, c).start()

    loads_b = [
        load(3 + i, far, near)
        for i, (far, near) in enumerate(
            ((normed_h, normed), (w_q_h, w_q), (w_g_h, w_g), (cot_h, cot))
        )
    ]

    def store_wait():
        for copy in loads_a:
            copy.wait()

    def table_wait():
        landed(tables.at[:st_n - 1], t_rs.at[0])

    store_wait()
    table_wait()

    def wanted(i, k):
        at = me_st * slots + k
        return tables[st_n - reach(i), at] if i else mine[at]

    def reach(i):
        return jnp.where(lax.rem(me_st, 2) == 0, st_n - i, i) if i else 0

    halves = (0, 1)

    def kv_copy(d, k):
        landing = arr_e.at[me_st * first + k] if k < first else arr_all.at[me_st * slots + k]
        source = served.at[d * slots + k]
        late = 0 if k < first else 1
        return remote(
            source, landing, kv_ss.at[late], kv_rs.at[late], (st_peer(reach(d)), me_tp)
        )

    def project(some):
        rows = jnp.concatenate([store[jnp.maximum(wanted(d, k), 0)] for d, k in some], axis=0)
        for half in halves:
            made = dot_nn(rows, (w_k, w_v)[half][...]).astype(BF16)
            for i, (d, k) in enumerate(some):
                piece = made[i * PLEN:(i + 1) * PLEN]
                if d:
                    served[d * slots + k, half] = piece
                elif k < first:
                    arr_e[me_st * first + k, half] = piece
                else:
                    arr_all[me_st * slots + k, half] = piece
        for d, k in some:
            if d and k < first:
                kv_copy(d, k).start()

    far = [(d, k) for k in range(slots) for d in range(1, st_n)]
    size = st_n - 1 if st_n <= GROUP else GROUP
    for i in range(0, len(far), size):
        project(far[i:i + size])
    near = [(0, k) for k in range(slots)]
    for i in range(0, slots, GROUP):
        project(near[i:i + GROUP])

    for d in range(st_n):
        for k in range(slots):
            served_ids[st_peer(reach(d)) * slots + k] = wanted(d, k)

    outs = []

    def put(i, near, far):
        copy = pltpu.make_async_copy(near, far, out_sem.at[i])
        copy.start()
        outs.append(copy)

    put(2, served_ids, served_out)
    for copy in loads_b:
        copy.wait()
    tile = 2 * BLK

    @pl.loop(0, tok // tile)
    def _(i):
        span = rows_at(i, tile)
        q_s[span, :] = dot_nn(normed[span, :], w_q[...]).astype(BF16)
        gate_s[span, :] = jax.nn.sigmoid(dot_nn(normed[span, :], w_g[...]))

    late = (st_n - 1) * (slots - first)

    def kv_arrived(phase):
        if phase == 0:
            landed(arr_e.at[:(st_n - 1) * first], kv_rs.at[0])
        else:
            landed(arr_all.at[:late], kv_rs.at[1])

    span = reads * PLEN

    def attend(b):
        if b == 0 or slots == first:
            parts = [arr_e[early_of[b * reads + r]] for r in range(reads)]
        else:
            parts = [arr_all[slot_of[b * reads + r]] for r in range(reads)]
        keys = jnp.concatenate([part[0] for part in parts], axis=0)
        values = jnp.concatenate([part[1] for part in parts], axis=0)
        toks = slice(b * BLK, (b + 1) * BLK)
        ctx = slice(b * span, (b + 1) * span)
        cols = [slice(h * DH, (h + 1) * DH) for h in range(heads)]
        colsv = [slice(hw + h * DH, hw + (h + 1) * DH) for h in range(heads)]
        k = [keys[:, ch] for ch in cols]
        v = [values[:, ch] for ch in cols]
        q = [q_s[toks, ch] for ch in cols]
        gate = [gate_s[toks, ch] for ch in cols]
        up = [cot[toks, ch].astype(F32) for ch in cols]
        each = range(heads)
        s = [dot_nt(q[h], k[h]) * scale for h in each]
        d_att = [(up[h] * gate[h]).astype(BF16) for h in each]
        d_p = [dot_nt(d_att[h], v[h]) for h in each]
        e = [jnp.exp(s[h] - jnp.max(s[h], axis=1, keepdims=True)) for h in each]
        p = [e[h] / jnp.sum(e[h], axis=1, keepdims=True) for h in each]
        low = [p[h].astype(BF16) for h in each]
        delta = [jnp.sum(d_p[h] * p[h], axis=1, keepdims=True) for h in each]
        d_s = [(p[h] * (d_p[h] - delta[h]) * scale).astype(BF16) for h in each]
        d_k = [dot_tn(d_s[h], q[h]) for h in each]
        d_v = [dot_tn(low[h], d_att[h]) for h in each]
        att = [dot_nn(low[h], v[h]) for h in each]
        d_q = [dot_nn(d_s[h], k[h]) for h in each]
        for h in each:
            dp_s[ctx, cols[h]] = d_k[h].astype(BF16)
            dp_s[ctx, colsv[h]] = d_v[h].astype(BF16)
        for h in each:
            dg_s[toks, cols[h]] = (up[h] * att[h] * gate[h] * (1.0 - gate[h])).astype(BF16)
            dq_s[toks, cols[h]] = d_q[h].astype(BF16)

    def chunk(g, t):
        which, b = g
        w_rows = rows_at(t, cw)
        if which == 0:
            ctx = slice(b * span, (b + 1) * span)
            return dot_nt(dp_s[ctx, :hw], w_k[w_rows, :]) + dot_nt(dp_s[ctx, hw:], w_v[w_rows, :])
        toks = slice(b * BLK, (b + 1) * BLK)
        return dot_nt(dq_s[toks, :], w_q[w_rows, :]) + dot_nt(dg_s[toks, :], w_g[w_rows, :])

    order = []
    for i in range((z_n + 1) // 2):
        order += [z_n - 1 - i, i] if z_n - 1 - i != i else [i]

    def piece_of(g, t):
        return (g[0] * blocks + g[1]) * z_n + t

    def all_of(g):
        at = piece_of(g, 0)
        return slice(at, at + z_n)

    batches = [[(0, 0)], [(1, 0)]] + [[(0, b)] for b in range(1, blocks)]
    batches.append([(1, b) for b in range(1, blocks)])
    early_groups = [g for batch in batches[:-1] for g in batch]

    def hop(g, t, up):
        n = piece_of(g, t)
        to = me_z + 1 if up else me_z - 1
        return remote(
            z_out.at[n], (up_in if up else dn_in).at[n],
            z_ss.at[0 if g in early_groups else 1],
            z_rs.at[piece_of(g, 0) // z_n * (z_n + 1) + t + (1 if up else 0)],
            (me_st, to * CORES + me_c),
        )

    def give(g):
        for t in order:
            x_out[piece_of(g, t)] = chunk(g, t * CORES + 1 - me_c).astype(BF16)
        i = piece_of(g, 0) // z_n
        for t in order:
            n = piece_of(g, t)
            remote(x_out.at[n], x_in.at[n], x_ss.at[0], x_rs.at[i], mate).start()

    def take(g):
        for t in order:
            own[piece_of(g, t)] = chunk(g, t * CORES + me_c)
        landed(x_in.at[all_of(g)], x_rs.at[piece_of(g, 0) // z_n])
        for t in order:
            n = piece_of(g, t)
            own[n] = own[n] + x_in[n].astype(F32)

    def depart(batch):
        @pl.when(me_z == 0)
        def _():
            for t in range(z_n - 1, 0, -1):
                for g in batch:
                    n = piece_of(g, t)
                    z_out[n] = own[n].astype(BF16)
                    hop(g, t, True).start()

        @pl.when(me_z == z_n - 1)
        def _():
            for t in range(z_n - 1):
                for g in batch:
                    n = piece_of(g, t)
                    z_out[n] = own[n].astype(BF16)
                    hop(g, t, False).start()

    def pass_on(batch, up, t):
        landing = up_in if up else dn_in
        for g in batch:
            n = piece_of(g, t)
            hop(g, t, up).wait_recv()
            z_out[n] = (own[n] + landing[n].astype(F32)).astype(BF16)
            hop(g, t, up).start()

    def relay(batch, z, stages):
        moves = [(z_n - 1 - t, z, True, t) for t in range(z + 1, z_n)]
        moves += [(t, z_n - 1 - z, False, t) for t in range(z)]
        moves = [m for m in moves if m[1] in stages]

        @pl.when(me_z == z)
        def _():
            for m in sorted(moves, key=lambda m: (m[0] + m[1], -m[1])):
                pass_on(batch, m[2], m[3])

    def gathered(g):
        n = piece_of(g, me_z)

        @pl.when(below)
        def _():
            hop(g, me_z, True).wait_recv()
            own[n] = own[n] + up_in[n].astype(F32)

        @pl.when(above)
        def _():
            hop(g, me_z, False).wait_recv()
            own[n] = own[n] + dn_in[n].astype(F32)

        which, b = g
        if which == 0:
            part[b * reads:(b + 1) * reads] = own[n].astype(BF16).reshape(reads, PLEN, cw)

    reads_end = blocks
    relayed = [0]

    def relay_step():
        j = relayed[0]
        relayed[0] += 1
        for z in range(1, z_n - 1):
            for k in range(1, z_n - 1):
                if 0 <= j - (k - 1) <= reads_end and k in (z, z_n - 1 - z):
                    relay(batches[j - (k - 1)], z, (k,))

    kv_arrived(0)
    for k in range(first, slots):
        for d in range(1, st_n):
            kv_copy(d, k).start()
    attend(0)
    give((0, 0))
    take((0, 0))
    depart(batches[0])
    give((1, 0))
    take((1, 0))
    depart(batches[1])
    if slots > first:
        for o in range(st_n):
            for k in range(first):
                arr_all[o * slots + k] = arr_e[o * first + k]
        kv_arrived(1)

    for b in range(1, blocks):
        attend(b)
        give((0, b))
        if b > 1:
            take((0, b - 1))
            depart([(0, b - 1)])
        if b == 2:
            relay_step()
    for b in range(1, blocks):
        give((1, b))
        if b == 1:
            take((0, blocks - 1))
            depart([(0, blocks - 1)])
            relay_step()
        else:
            take((1, b - 1))
    take((1, blocks - 1))
    depart(batches[-1])
    relay_step()

    dw = depth // st_n
    for d in list(range(1, st_n)) + [0]:
        term = dot_tn(normed[:, rows_at(st_peer(d), dw)], dq_s[...])
        if d == 0:
            g_own[...] = term
        else:
            g_out[d] = term.astype(BF16)
            remote(
                g_out.at[d], g_in.at[d], g_ss.at[0], g_rs.at[0], (st_peer(d), me_tp)
            ).start()

    while relayed[0] < reads_end + 1 + max(z_n - 3, 0):
        relay_step()
    for b in range(blocks):
        gathered((0, b))
    for s in range(st_n * slots):
        r_out[s] = part[req_of[s]]
    for d in range(1, st_n):
        reader = st_peer(reach(d))
        remote(
            r_out.at[rows_at(reader, slots)], r_in.at[rows_at(me_st, slots)],
            r_ss.at[0], r_rs.at[0], (reader, me_tp),
        ).start()
    r_in[rows_at(me_st, slots)] = r_out[rows_at(me_st, slots)]

    def gqw_wait():
        total = g_own[...]
        landed(g_in.at[:st_n - 1], g_rs.at[0])
        for d in range(1, st_n):
            total = total + g_in[d].astype(F32)
        g_own[...] = total
        put(1, g_own, gqw_out)

    def send_wait():
        gone(served.at[:(st_n - 1) * first], kv_ss.at[0])
        if slots > first:
            gone(served.at[:late], kv_ss.at[1])
        gone(x_out, x_ss.at[0])
        gone(g_out.at[:st_n - 1], g_ss.at[0])
        gone(z_out.at[:len(early_groups) * (z_n - 1)], z_ss.at[0])

    @pl.when(me_c == CORES - 1)
    def _():
        for c in range(CORES):
            gone(tables.at[:st_n - 1], t_ss.at[c])

    for z in range(1, z_n - 1):
        relay(batches[-1], z, range(z_n))
    gqw_wait()
    send_wait()

    def ret_wait():
        landed(r_in.at[:(st_n - 1) * slots], r_rs.at[0])
        put(0, r_in, ret_out)

    ret_wait()
    for b in range(blocks):
        gathered((1, b))
        put(3 + b, own.at[piece_of((1, b), me_z)], rows_out.at[b * BLK:(b + 1) * BLK])
    gone(z_out.at[:len(batches[-1]) * (z_n - 1)], z_ss.at[1])
    gone(r_out.at[:(st_n - 1) * slots], r_ss.at[0])

    def out_wait():
        for copy in outs:
            copy.wait()

    out_wait()


def main_call(st_n, tp_n, ids, store, normed, w_q, w_g, w_k, w_v, cot):
    reads, blocks = ids.shape
    tok, hw = cot.shape
    depth = w_q.shape[0]
    cw, dw, z_n = depth // tp_n, depth // st_n, tp_n // CORES
    pass_dev = store.shape[0]
    n_pos = blocks * reads
    slots = max(1, 2 * n_pos // st_n)
    first = min(reads, slots)
    ctx = blocks * reads * PLEN
    slot_total = st_n * slots
    hbm = pl.BlockSpec(memory_space=pl.ANY)
    pieces = 2 * blocks * z_n
    piece = lambda kind=BF16: pltpu.VMEM((pieces, BLK, cw), kind)
    sem = lambda n: pltpu.SemaphoreType.DMA((n,))
    table = lambda *n: pltpu.SMEM(n, jnp.int32)
    assert ctx == tok
    return pl.pallas_call(
        functools.partial(main_kernel, st_n, tp_n, reads, slots, pass_dev),
        out_shape=(
            jax.ShapeDtypeStruct((tok, cw), F32),
            jax.ShapeDtypeStruct((slot_total, PLEN, cw), BF16),
            jax.ShapeDtypeStruct((dw, hw), F32),
            jax.ShapeDtypeStruct((slot_total,), jnp.int32),
        ),
        in_specs=[hbm] * 8,
        out_specs=(hbm, hbm, hbm, hbm),
        scratch_shapes=[
            *[pltpu.VMEM(a.shape, a.dtype) for a in (store, normed, w_q, w_g, w_k, w_v, cot)],
            sem(8),
            table(*ids.shape), table(slot_total), table(st_n, slot_total), table(slot_total),
            table(slot_total), table(n_pos), table(n_pos),
            sem(CORES), sem(1),
            pltpu.VMEM((slot_total, 2, PLEN, hw), BF16),
            pltpu.VMEM((st_n * first, 2, PLEN, hw), BF16),
            pltpu.VMEM((slot_total, 2, PLEN, hw), BF16),
            pltpu.VMEM((tok, hw), BF16),
            pltpu.VMEM((tok, hw), F32),
            pltpu.VMEM((tok, hw), BF16),
            pltpu.VMEM((tok, hw), BF16),
            pltpu.VMEM((ctx, 2 * hw), BF16),
            piece(), piece(), piece(), piece(), piece(), piece(F32),
            pltpu.VMEM((ctx // PLEN, PLEN, cw), BF16),
            pltpu.VMEM((slot_total, PLEN, cw), BF16),
            pltpu.VMEM((slot_total, PLEN, cw), BF16),
            pltpu.VMEM((st_n, dw, hw), BF16),
            pltpu.VMEM((st_n, dw, hw), BF16),
            pltpu.VMEM((dw, hw), F32),
            sem(2), sem(2), sem(1), sem(2 * blocks), sem(2), sem(2 * blocks * (z_n + 1)),
            sem(1), sem(1), sem(1), sem(1), sem(3 + blocks),
        ],
        compiler_params=pltpu.CompilerParams(
            collective_id=0, has_side_effects=True, vmem_limit_bytes=46 << 20
        ),
        name="main",
    )(*[
        pltpu.with_memory_space_constraint(a, pltpu.HBM)
        for a in (ids, store, normed, w_q, w_g, w_k, w_v, cot)
    ])


def spread_kernel(
    ids_h, returned, rows, gqw, out_h, rows_out, gqw_out, ids, total, sems, chunk_sem,
):
    slots, passes = ids.shape[0], out_h.shape[0]
    names = pltpu.make_async_copy(ids_h, ids, sems.at[2])
    names.start()
    outs = [
        pltpu.make_async_copy(near, far, sems.at[i])
        for i, (near, far) in enumerate(((rows, rows_out), (gqw, gqw_out)))
    ]
    for copy in outs:
        copy.start()
    total[...] = jnp.zeros_like(total)
    names.wait()
    for s in range(slots):

        @pl.when(ids[s] >= 0)
        def _():
            total[ids[s]] += returned[s].astype(F32)

    chunks = chunk_sem.shape[0]
    size = passes // chunks
    for i in range(chunks):
        span = slice(i * size, (i + 1) * size)
        outs.append(pltpu.make_async_copy(total.at[span], out_h.at[span], chunk_sem.at[i]))
        outs[-1].start()
    for copy in outs:
        copy.wait()


def spread(ids, returned, grad_rows, grad_query_weight, passes):
    width = returned.shape[2]
    hbm = pl.BlockSpec(memory_space=pl.ANY)
    vmem = pl.BlockSpec(memory_space=pltpu.VMEM)
    chunks = GROUP if passes % GROUP == 0 else 1
    return pl.pallas_call(
        spread_kernel,
        out_shape=(
            jax.ShapeDtypeStruct((passes, PLEN, width), F32),
            jax.ShapeDtypeStruct(grad_rows.shape, F32),
            jax.ShapeDtypeStruct(grad_query_weight.shape, F32),
        ),
        in_specs=[hbm] + [vmem] * 3,
        out_specs=(hbm,) * 3,
        scratch_shapes=[
            pltpu.SMEM(ids.shape, jnp.int32),
            pltpu.VMEM((passes, PLEN, width), F32),
            pltpu.SemaphoreType.DMA((3,)),
            pltpu.SemaphoreType.DMA((chunks,)),
        ],
        compiler_params=pltpu.CompilerParams(vmem_limit_bytes=8 << 20),
        name="spread",
    )(ids, returned, grad_rows, grad_query_weight)


def shards(normed, store, passage_ids, w_query, w_gate, w_key, w_value, cotangent):
    grad_rows, returned, grad_query_weight, served_ids = main_call(
        lax.axis_size("st"), lax.axis_size("tp"), passage_ids.T,
        store.reshape(-1, PLEN, store.shape[1]), normed, w_query, w_gate, w_key, w_value, cotangent,
    )
    grad_store, grad_rows, grad_query_weight = spread(
        served_ids, returned, grad_rows, grad_query_weight, store.shape[0] // PLEN
    )
    return (grad_rows, grad_store.reshape(store.shape[0], -1), grad_query_weight)


def solution(mesh):
    placed = (
        P("st", None),
        P("st", None),
        P("st", None),
        P(None, "tp"),
        P(None, "tp"),
        P(None, "tp"),
        P(None, "tp"),
        P("st", "tp"),
    )
    return jax.shard_map(
        shards,
        mesh=mesh,
        in_specs=placed,
        out_specs=(P("st", "tp"), P("st", "tp"), P("st", "tp")),
        check_vma=False,
    )
```
